32 devices in a mesh: grp: 2 (over y), sp: 4 (over z), fs: 2 (over x), tp: 2 (over core).
Axes of the slice: x: 2, y: 2, z: 4, core: 2. Of those that a mesh axis runs over, the one named last changes fastest.
Arguments:
- tokens: bfloat16 [4, 512, 2048], P(('grp', 'fs'), 'sp'), parts along dimension 0, may hold values from -6 to 6
- norm_gain: float32 [2048], replicated, may hold values from 0.1 to 1.9
- query_attend: bfloat16 [2048, 8, 128], P(None, ('fs', 'tp')), may hold values from -0.125 to 0.125
- key_attend: bfloat16 [2048, 8, 128], P(None, ('fs', 'tp')), may hold values from -0.125 to 0.125
- value_attend: bfloat16 [2048, 8, 128], P(None, ('fs', 'tp')), may hold values from -0.125 to 0.125
- query_linear: bfloat16 [2048, 8, 128], P(None, ('fs', 'tp')), may hold values from -0.125 to 0.125
- key_linear: bfloat16 [2048, 8, 128], P(None, ('fs', 'tp')), may hold values from -0.125 to 0.125
- value_linear: bfloat16 [2048, 8, 256], P(None, ('fs', 'tp')), may hold values from -0.125 to 0.125
- decay_down: bfloat16 [2048, 32], replicated, may hold values from -0.125 to 0.125
- decay_up: bfloat16 [32, 8, 128], replicated, may hold values from -2.109375 to 2.109375
- decay_bias: float32 [8, 128], replicated, may hold values from -1.5 to 7.5
- log_retain: float32 [4, 512, 8], P(('grp', 'fs'), 'sp'), parts along dimension 0, may hold values from -1.5 to 0
- query_gain: float32 [64], replicated, may hold values from 0.6 to 4
- key_gain: float32 [8, 2, 64], replicated, may hold values from 0.8 to 14
- diff_lambda: float32 [8], replicated, may hold values from 0.3 to 0.8
- mix_gain: float32 [128], replicated, may hold values from 0.1 to 1.9
- state_gain: float32 [256], replicated, may hold values from 0.1 to 1.9
- init_state: float32 [4, 8, 128, 256], P('grp', ('fs', 'tp')), parts along dimension 0, may hold values from -80 to 80
- output_attend: bfloat16 [1024, 2048], P(None, 'tp'), may hold values from -0.109375 to 0.109375
- output_linear: bfloat16 [2048, 2048], P(None, 'tp'), may hold values from -0.109375 to 0.109375
Outputs:
- mixed_out: bfloat16 [4, 512, 2048], P(('grp', 'fs'), 'sp', 'tp'), parts along dimension 0
The draws below stay inside these ranges and needn't reach their ends.
There are 2 independent parts, one for each index of `grp`. The reference program is written for one: setup_inputs(seed, part) draws one part's arguments, and reference() takes and returns one part's arrays. A program takes and returns all parts, laid end to end along the dimension named above; an argument that names none is the same for every part. Nothing has to cross between parts.
All inputs are finite; a program needn't handle non-finite values.
Results may differ from the reference program's by a relative error of at most 0.018.
The reference program's roundings to bfloat16 on the way count: a program that leaves them out, or rounds other values in their place, can miss the bound.
Values may be sent and summed in bfloat16 or wider, within the bound.
No kernel may reach another device: no remote copies, remote signals or barrier semaphores. Data moves between devices by JAX's collectives and lax.ppermute only.
A program may use at most 128 MiB of HBM per device.

```python
import math
import jax
import jax.numpy as jnp
from jax import lax

D = 2048
MIXER_HEADS = 8
HD_A = 64
DV_A = 128
HDK = 128
HDV = 256
RANK = 32
BLK = 64
TOK_DEV = 128
SEQUENCE_LENGTH = 512
SEQUENCE_COUNT = 2
N_SP = 4


def draw_query_gain(key, part):
    return jax.random.uniform(key, (HD_A,), jnp.float32, 0.6, 2.0)


def draw_key_gain(key, part):
    level_key = jax.random.fold_in(key, 11)
    channel_key = jax.random.fold_in(key, 12)
    level = jax.random.uniform(level_key, (MIXER_HEADS, 2, 1), jnp.float32, 1.2, 1.6)
    return level * jax.random.uniform(channel_key, (MIXER_HEADS, 2, HD_A), jnp.float32, 0.85, 1.15)


def draw_decay_bias(key, part):
    pick_key = jax.random.fold_in(key, 21)
    fast_key = jax.random.fold_in(key, 22)
    slow_key = jax.random.fold_in(key, 23)
    share = 0.5
    fast_pick = jax.random.uniform(pick_key, (MIXER_HEADS, HDK), jnp.float32) < share
    fast_value = jax.random.uniform(fast_key, (MIXER_HEADS, HDK), jnp.float32, -1.5, 0.5)
    slow_value = jax.random.uniform(slow_key, (MIXER_HEADS, HDK), jnp.float32, 6.0, 7.5)
    return jnp.where(fast_pick, fast_value, slow_value)


def draw_log_retain(key, part):
    rate_key = jax.random.fold_in(key, 31)
    spot_key = jax.random.fold_in(key, 32)
    random_depth_key = jax.random.fold_in(key, 33)
    block_total = SEQUENCE_LENGTH // TOK_DEV
    factor = jnp.exp(jax.random.uniform(rate_key, (SEQUENCE_COUNT, block_total, 1, MIXER_HEADS), jnp.float32, math.log(0.5), math.log(2.0)))
    position_offset = jnp.broadcast_to(-0.8 / SEQUENCE_LENGTH * factor, (SEQUENCE_COUNT, block_total, TOK_DEV, MIXER_HEADS)).reshape(SEQUENCE_COUNT, SEQUENCE_LENGTH, MIXER_HEADS)
    spike_positions = jax.random.randint(spot_key, (SEQUENCE_COUNT, 1, MIXER_HEADS, 2), 0, SEQUENCE_LENGTH)
    spike_depth = jnp.log(jax.random.uniform(random_depth_key, (SEQUENCE_COUNT, 1, MIXER_HEADS, 2), jnp.float32, 0.5, 0.8))
    spike_location = jnp.arange(SEQUENCE_LENGTH, dtype=jnp.int32)[None, :, None, None] == spike_positions
    spike_total = jnp.sum(jnp.where(spike_location, spike_depth, 0.0), axis=-1)
    return position_offset + spike_total


def shard_levels(key, extent, shards, smallest, high):
    loudness, own = 1.0, jax.random.fold_in(key, 6)
    for dim, blocks in shards:
        draws = jnp.exp(jax.random.uniform(jax.random.fold_in(own, dim), (blocks,), jnp.float32, smallest / len(shards), high / len(shards)))
        loudness = loudness * jnp.repeat(draws, extent[dim] // blocks).reshape([-1 if axis == dim else 1 for axis in range(len(extent))])
    return loudness


def normal_values(own_key, shape, width, reach, split=(), kind=jnp.bfloat16):
    result = jax.random.normal(own_key, shape, jnp.float32) * width
    if len(split) > 0:
        result = shard_levels(own_key, shape, split, -0.22, 0.18) * result
    return jnp.clip(result, min=-reach, max=reach).astype(kind)


def setup_inputs(seed: int = 0, part: int = 0) -> dict:
    arg_keys = jax.random.split(jax.random.key(seed), 21)
    part_splits = jax.random.split(jax.random.fold_in(arg_keys[20], part), 21)
    tokens = normal_values(part_splits[0], (SEQUENCE_COUNT, SEQUENCE_LENGTH, D), 1.0, 6.0, ((0, 2), (1, 4)))
    norm_gain = jnp.clip(1.0 + 0.18 * jax.random.normal(arg_keys[1], (D,), jnp.float32), 0.1, 1.9)
    query_attend = normal_values(arg_keys[2], (D, MIXER_HEADS, 2 * HD_A), D ** -0.5, 0.125, ((1, 4),))
    key_attend = normal_values(arg_keys[3], (D, MIXER_HEADS, 2 * HD_A), D ** -0.5, 0.125, ((1, 4),))
    value_attend = normal_values(arg_keys[4], (D, MIXER_HEADS, DV_A), D ** -0.5, 0.125, ((1, 4),))
    query_linear = normal_values(arg_keys[5], (D, MIXER_HEADS, HDK), D ** -0.5, 0.125, ((1, 4),))
    key_linear = normal_values(arg_keys[6], (D, MIXER_HEADS, HDK), D ** -0.5, 0.125, ((1, 4),))
    value_linear = normal_values(arg_keys[7], (D, MIXER_HEADS, HDV), D ** -0.5, 0.125, ((1, 4),))
    decay_down = normal_values(arg_keys[8], (D, RANK), D ** -0.5, 0.125)
    decay_up = normal_values(arg_keys[9], (RANK, MIXER_HEADS, HDK), (2.0 / RANK ** 0.5), 2.109375)
    decay_bias = draw_decay_bias(jax.random.fold_in(arg_keys[20], 71), part)
    log_retain = draw_log_retain(jax.random.fold_in(jax.random.fold_in(arg_keys[20], part), 71), part)
    query_gain = draw_query_gain(jax.random.fold_in(arg_keys[20], 71), part)
    key_gain = draw_key_gain(jax.random.fold_in(arg_keys[20], 71), part)
    diff_lambda = jnp.clip(jax.random.uniform(arg_keys[14], (MIXER_HEADS,), jnp.float32, 0.3, 0.8), 0.3, 0.8)
    mix_gain = jnp.clip(1.0 + 0.18 * jax.random.normal(arg_keys[15], (DV_A,), jnp.float32), 0.1, 1.9)
    state_gain = jnp.clip(1.0 + 0.18 * jax.random.normal(arg_keys[16], (HDV,), jnp.float32), 0.1, 1.9)
    init_state = normal_values(part_splits[17], (SEQUENCE_COUNT, MIXER_HEADS, HDK, HDV), (0.6 * (TOK_DEV * N_SP) ** 0.5), 80.0, ((1, 4),), jnp.float32)
    output_attend = normal_values(arg_keys[18], (MIXER_HEADS * DV_A, D), (MIXER_HEADS * (DV_A + HDV)) ** -0.5, 0.109375, ((1, 2),))
    output_linear = normal_values(arg_keys[19], (MIXER_HEADS * HDV, D), (MIXER_HEADS * (DV_A + HDV)) ** -0.5, 0.109375, ((1, 2),))
    return dict(tokens=tokens, norm_gain=norm_gain, query_attend=query_attend, key_attend=key_attend, value_attend=value_attend, query_linear=query_linear, key_linear=key_linear, value_linear=value_linear, decay_down=decay_down, decay_up=decay_up, decay_bias=decay_bias, log_retain=log_retain, query_gain=query_gain, key_gain=key_gain, diff_lambda=diff_lambda, mix_gain=mix_gain, state_gain=state_gain, init_state=init_state, output_attend=output_attend, output_linear=output_linear)


norm_eps = 1e-06
decay_tau = 16.0

def rms_scale(values, gain):
    widened = values.astype(jnp.float32)
    return widened * lax.rsqrt(lax.optimization_barrier(jnp.mean(widened * widened, axis=-1, keepdims=True)) + norm_eps) * gain

def widen(values):
    return lax.optimization_barrier(values).astype(jnp.float32)

def gated_linear(queries, keys_in, values_in, log_decay, first_state):
    length, head_count, key_dim = queries.shape
    block_count = length // BLK
    highest_precision = lax.Precision.HIGHEST

    def split_blocks(source):
        return source.reshape(block_count, BLK, head_count, source.shape[-1])
    causal = (jnp.arange(BLK, dtype=jnp.int32)[:, None] >= jnp.arange(BLK, dtype=jnp.int32)[None, :])[None]

    def advance(recurrent_state, inputs_now):
        question_patch_lines, block_k, value_tile_width, block_log = inputs_now
        running_state = jnp.cumsum(block_log, axis=0)
        pivot = running_state[BLK // 2]
        q_scaled = question_patch_lines * jnp.exp(running_state - pivot[None])
        k_scaled = block_k * jnp.exp(pivot[None] - running_state)
        scores = jnp.einsum('thk,shk->hts', q_scaled, k_scaled, precision=highest_precision)
        scores = jnp.where(causal, scores, 0.0)
        inside_block = jnp.einsum('hts,shv->thv', scores, value_tile_width, precision=highest_precision)
        inside_block = inside_block + jnp.einsum('jwo,wos->jws', question_patch_lines * jnp.exp(running_state), recurrent_state, precision=highest_precision)
        final_state = running_state[-1]
        faded_memory_matrix = block_k * jnp.exp(final_state[None] - running_state)
        recurrent_state = recurrent_state * jnp.exp(final_state)[:, :, None] + jnp.einsum('zcb,zcw->cbw', faded_memory_matrix, value_tile_width, precision=highest_precision)
        return (recurrent_state, inside_block)
    _, outputs = lax.scan(advance, first_state, (split_blocks(queries), split_blocks(keys_in), split_blocks(values_in), split_blocks(log_decay)))
    return outputs.reshape(length, head_count, values_in.shape[-1])

def reference(tokens, norm_gain, query_attend, key_attend, value_attend, query_linear, key_linear, value_linear, decay_down, decay_up, decay_bias, log_retain, query_gain, key_gain, diff_lambda, mix_gain, state_gain, init_state, output_attend, output_linear):

    def one_sequence(inputs_now):
        seq_tokens, seq_retain, seq_state = inputs_now
        seq_len = seq_tokens.shape[0]
        normed = rms_scale(seq_tokens, norm_gain).astype(jnp.bfloat16)

        def project(weight):
            return jnp.dot(normed, weight.reshape(weight.shape[0], -1), preferred_element_type=jnp.float32).astype(jnp.bfloat16)
        q_unit = rms_scale(project(query_attend).reshape(seq_len, MIXER_HEADS, 2, HD_A), query_gain).astype(jnp.bfloat16)
        k_unit = rms_scale(project(key_attend).reshape(seq_len, MIXER_HEADS, 2, HD_A), key_gain).astype(jnp.bfloat16)
        v_attend = project(value_attend).reshape(seq_len, MIXER_HEADS, DV_A)
        key_wide = widen(k_unit)
        value_wide = widen(v_attend)
        position_block = jnp.arange(seq_len, dtype=jnp.int32) // BLK

        def attend(block_index):
            first_row = (block_index * TOK_DEV).astype(jnp.int32)
            query_rows = widen(lax.dynamic_slice_in_dim(q_unit, first_row, TOK_DEV, 0))
            query_block = lax.dynamic_slice_in_dim(position_block, first_row, TOK_DEV, 0)
            scores = jnp.einsum('qhmd,khmd->hmqk', query_rows, key_wide) * HD_A ** (-0.5)
            allowed = query_block[:, None] >= position_block[None, :]
            scores = jnp.where(allowed, scores, -jnp.inf)
            top = lax.optimization_barrier(jnp.max(scores, axis=-1, keepdims=True))
            raised = jnp.exp(scores - top)
            totals = lax.optimization_barrier(jnp.sum(raised, axis=-1))
            sums = jnp.einsum('hmqk,khv->hmqv', widen(raised.astype(jnp.bfloat16)), value_wide)
            return sums[:, 0] / totals[:, 0, :, None] - diff_lambda[:, None, None] * sums[:, 1] / totals[:, 1, :, None]
        diff_raw = lax.map(attend, jnp.arange(seq_len // TOK_DEV, dtype=jnp.int32))
        diff_raw = jnp.transpose(diff_raw, (0, 2, 1, 3)).reshape(seq_len, MIXER_HEADS, DV_A)
        attend_out = rms_scale(diff_raw, mix_gain).astype(jnp.bfloat16)
        q_lin = project(query_linear).reshape(seq_len, MIXER_HEADS, HDK)
        k_lin = project(key_linear).reshape(seq_len, MIXER_HEADS, HDK)
        v_lin = project(value_linear).reshape(seq_len, MIXER_HEADS, HDV)
        low_rank = jnp.dot(normed, decay_down, preferred_element_type=jnp.float32).astype(jnp.bfloat16)
        pre_act = jnp.dot(low_rank, decay_up.reshape(RANK, -1), preferred_element_type=jnp.float32).reshape(seq_len, MIXER_HEADS, HDK) + decay_bias
        log_decay = jax.nn.log_sigmoid(pre_act) / decay_tau + seq_retain[:, :, None]
        linear_raw = gated_linear(widen(q_lin) * HDK ** (-0.5), widen(k_lin), widen(v_lin), log_decay, seq_state)
        linear_out = rms_scale(linear_raw, state_gain).astype(jnp.bfloat16)
        total = jnp.dot(attend_out.reshape(seq_len, -1), output_attend, preferred_element_type=jnp.float32)
        total = total + jnp.dot(linear_out.reshape(seq_len, -1), output_linear, preferred_element_type=jnp.float32)
        return total.astype(jnp.bfloat16)
    return lax.map(one_sequence, (tokens, log_retain, init_state))
```

```python
import functools

import jax
import jax.numpy as jnp
from jax import lax
from jax.experimental import pallas as pl
from jax.experimental.pallas import tpu as pltpu
from jax.sharding import PartitionSpec as P

EPS = 1e-06
TAU = 16.0
BLK = 64
F32 = jnp.float32
BF16 = jnp.bfloat16
HIGH = lax.Precision.HIGHEST


def dot(a, b, dims=((1,), (0,)), precision=None):
    return lax.dot_general(a, b, (dims, ((), ())), precision=precision, preferred_element_type=F32)


def rms(x, gain):
    return x * lax.rsqrt(jnp.mean(x * x, axis=-1, keepdims=True) + EPS) * gain


def rms_halves(x, gain):
    rows, width = x.shape
    half = width // 2
    first = lax.broadcasted_iota(jnp.int32, x.shape, 1) < half
    sq = x * x
    low = jnp.sum(jnp.where(first, sq, 0.0), axis=-1, keepdims=True) / half
    high = jnp.sum(jnp.where(first, 0.0, sq), axis=-1, keepdims=True) / half
    return x * jnp.where(first, lax.rsqrt(low + EPS), lax.rsqrt(high + EPS)) * gain


def whole(shape, memory_space=pltpu.VMEM):
    return pl.BlockSpec(shape, lambda *_: (0,) * len(shape), memory_space=memory_space)


SMEM = pl.BlockSpec(memory_space=pltpu.SMEM)


def unpack_weight(w_ref, wide_ref, heads, parts, out_ref, column):
    rows = w_ref.shape[0] // (heads * parts)
    if heads * parts == 1:
        out_ref[:, column : column + 128] = w_ref[...]
        return
    wide_ref[: w_ref.shape[0], :] = w_ref[...].astype(F32)
    for head in range(heads):
        for part in range(parts):
            piece = wide_ref[pl.ds(part * heads + head, rows, stride=heads * parts), :]
            at = column + (head * parts + part) * 128
            out_ref[:, at : at + 128] = piece.astype(BF16)


class Dims:
    def __init__(self, tokens, query_attend, value_attend, key_linear, value_linear, decay_up):
        self.rows = tokens.shape[1]
        self.model = tokens.shape[2]
        self.heads = query_attend.shape[1]
        self.ca = query_attend.shape[2]
        self.va = value_attend.shape[2]
        self.ck = key_linear.shape[2]
        self.cv = value_linear.shape[2]
        self.all_heads = decay_up.shape[1]
        self.rank = decay_up.shape[0]
        self.kv = self.heads * (self.ca + self.va)
        self.rest = self.heads * (self.ca + 2 * self.ck + self.cv)
        self.steps = 4
        self.chunk = self.model // self.steps


def norm_into(parts, start_of, gain, normed_ref):
    for index, part in enumerate(parts):
        values = rms(part[...].astype(F32), gain[...]).astype(BF16)
        normed_ref[pl.ds(start_of(index), part.shape[0]), :] = values


def write_kv(acc, key_gain, meta, dims, out):
    for h in range(dims.heads):
        k = acc[:, h * dims.ca : (h + 1) * dims.ca].astype(BF16).astype(F32)
        row = 2 * (meta[1] + h)
        gain = jnp.concatenate([key_gain[pl.ds(row, 1), :], key_gain[pl.ds(row + 1, 1), :]], axis=1)
        out[:, h * dims.ca : (h + 1) * dims.ca] = rms_halves(k, gain).astype(BF16)
    at = dims.heads * dims.ca
    out[:, at:] = acc[:, at:].astype(BF16)


def kv_first(dims, tokens, gain, wk, wv, key_gain, meta):
    hd = dims.heads

    def body(meta_ref, tok, gain_ref, wk_ref, wv_ref, kg, kv_out, normed_out, w_out, acc, wide):
        step = pl.program_id(0)

        @pl.when(step == 0)
        def _():
            norm_into([tok], lambda i: 0, gain_ref, normed_out)
            acc[...] = jnp.zeros_like(acc)

        unpack_weight(wk_ref, wide, hd, dims.ca // 128, w_out, 0)
        unpack_weight(wv_ref, wide, hd, dims.va // 128, w_out, hd * dims.ca)
        at = pl.multiple_of(step * dims.chunk, dims.chunk)
        acc[...] += dot(normed_out[:, pl.ds(at, dims.chunk)], w_out[...])

        @pl.when(step == dims.steps - 1)
        def _():
            write_kv(acc[...], kg, meta_ref, dims, kv_out)

    return pl.pallas_call(
        body,
        grid=(dims.steps,),
        in_specs=[
            SMEM,
            whole(tokens.shape),
            whole(gain.shape),
            pl.BlockSpec((wk.shape[0] // dims.steps, 128), lambda i: (i, 0)),
            pl.BlockSpec((wv.shape[0] // dims.steps, 128), lambda i: (i, 0)),
            whole(key_gain.shape),
        ],
        out_specs=[
            whole((dims.rows, dims.kv)),
            whole((dims.rows, dims.model)),
            pl.BlockSpec((dims.chunk, dims.kv), lambda i: (i, 0)),
        ],
        out_shape=[
            jax.ShapeDtypeStruct((dims.rows, dims.kv), BF16),
            jax.ShapeDtypeStruct((dims.rows, dims.model), BF16),
            jax.ShapeDtypeStruct((dims.model, dims.kv), BF16),
        ],
        scratch_shapes=[
            pltpu.VMEM((dims.rows, dims.kv), F32),
            pltpu.VMEM((wk.shape[0] // dims.steps, 128), F32),
        ],
        name="kv_first",
    )(meta, tokens, gain, wk, wv, key_gain)


def kv_other(dims, parts, gain, weights, key_gain, meta):
    count = len(parts)
    piece = parts[0].shape[0]

    def body(meta_ref, *refs):
        toks, (gain_ref, w_ref, kg, kv_out, normed_out) = refs[:count], refs[count:]
        norm_into(toks, lambda i: lax.rem(meta_ref[2] + i, count) * piece, gain_ref, normed_out)
        write_kv(dot(normed_out[...], w_ref[...]), kg, meta_ref, dims, kv_out)

    return pl.pallas_call(
        body,
        in_specs=[SMEM] + [whole(p.shape) for p in parts] + [whole(gain.shape), whole(weights.shape), whole(key_gain.shape)],
        out_specs=[whole((dims.rows, dims.kv)), whole((dims.rows, dims.model))],
        out_shape=[
            jax.ShapeDtypeStruct((dims.rows, dims.kv), BF16),
            jax.ShapeDtypeStruct((dims.rows, dims.model), BF16),
        ],
        name="kv_other",
    )(meta, *parts, gain, weights, key_gain)


def rest_outputs(dims):
    hd, rows = dims.heads, dims.rows
    return [
        jax.ShapeDtypeStruct((rows, hd * dims.ca), BF16),
        jax.ShapeDtypeStruct((rows, hd * dims.ck), BF16),
        jax.ShapeDtypeStruct((rows, hd * dims.cv), F32),
        jax.ShapeDtypeStruct((hd * dims.ck + 16, dims.cv), BF16),
        jax.ShapeDtypeStruct((hd * dims.ck, dims.cv), F32),
        jax.ShapeDtypeStruct((16, dims.ck), F32),
    ]


def local_part(dims, acc, low_rank, meta, slot_state, up, up_wide, bias, retain, query_gain, outs):
    q_out, reach_out, inside_out, send_out, state_out, decay_out = outs
    hd, rows, ck, cv = dims.heads, dims.rows, dims.ck, dims.cv
    gain = jnp.concatenate([query_gain[...], query_gain[...]], axis=1)
    up_wide[...] = up[...].astype(F32)
    retain_columns = jnp.transpose(retain[...])
    head_lane = lax.broadcasted_iota(jnp.int32, retain_columns.shape, 1)
    row_id = lax.broadcasted_iota(jnp.int32, (rows, rows), 0)
    col_id = lax.broadcasted_iota(jnp.int32, (rows, rows), 1)
    same_block = row_id // BLK == col_id // BLK
    lower = row_id >= col_id
    summing = jnp.where(same_block & lower, 1.0, 0.0).astype(F32)
    blocks = rows // BLK
    first = meta[0] == 0
    send_out[hd * ck :, :] = jnp.zeros((16, cv), BF16)
    decay_out[...] = jnp.ones((16, ck), F32)
    for h in range(hd):
        q = acc[:, h * dims.ca : (h + 1) * dims.ca].astype(BF16).astype(F32)
        q_out[:, h * dims.ca : (h + 1) * dims.ca] = rms_halves(q, gain).astype(BF16)
        at = hd * dims.ca + h * ck
        ql = acc[:, at : at + ck].astype(BF16).astype(F32) * ck ** (-0.5)
        at = hd * (dims.ca + ck) + h * ck
        kl = acc[:, at : at + ck].astype(BF16).astype(F32)
        at = hd * (dims.ca + 2 * ck) + h * cv
        vl = acc[:, at : at + cv].astype(BF16)
        head = meta[1] + h
        up_head = up_wide[pl.ds(head, dims.rank, stride=dims.all_heads), :].astype(BF16)
        pre = dot(low_rank, up_head) + bias[pl.ds(head, 1), :]
        gate = jnp.minimum(pre, 0.0) - jnp.log1p(jnp.exp(-jnp.abs(pre)))
        kept = jnp.sum(jnp.where(head_lane == head, retain_columns, 0.0), axis=1, keepdims=True)
        log_decay = gate / TAU + kept
        running = dot(summing, log_decay, precision=HIGH)
        finals = [running[(b + 1) * BLK - 1 : (b + 1) * BLK, :] for b in range(blocks)]
        pivots = [running[b * BLK + BLK // 2 : b * BLK + BLK // 2 + 1, :] for b in range(blocks)]
        q_blocks, reach_blocks, k_ends, inside = [], [], [], []
        before = jnp.zeros_like(finals[0])
        for b in range(blocks):
            here = slice(b * BLK, (b + 1) * BLK)
            run = running[here]
            q_edge = ql[here] * jnp.exp(run)
            q_piv = (ql[here] * jnp.exp(run - pivots[b])).astype(BF16)
            k_piv = (kl[here] * jnp.exp(pivots[b] - run)).astype(BF16)
            own = dot(q_piv, k_piv, ((1,), (1,)))
            own = jnp.where(lower[:BLK, :BLK], own, 0.0).astype(BF16)
            result = dot(own, vl[here])
            gap = jnp.zeros_like(finals[0])
            for c in range(b - 1, -1, -1):
                across = dot(q_edge.astype(BF16), (k_ends[c] * jnp.exp(gap)).astype(BF16), ((1,), (1,)))
                result = result + dot(across.astype(BF16), vl[c * BLK : (c + 1) * BLK])
                gap = gap + finals[c]
            inside.append(result)
            reach_blocks.append((q_edge * jnp.exp(before)).astype(BF16))
            k_ends.append(kl[here] * jnp.exp(finals[b] - run))
            before = before + finals[b]
        for b in range(blocks):
            here = slice(b * BLK, (b + 1) * BLK)
            inside_out[here, h * cv : (h + 1) * cv] = inside[b]
            reach_out[here, h * ck : (h + 1) * ck] = reach_blocks[b]
        later = jnp.zeros_like(finals[0])
        faded = [None] * blocks
        for b in range(blocks - 1, -1, -1):
            faded[b] = (k_ends[b] * jnp.exp(later)).astype(BF16)
            later = later + finals[b]
        state = dot(jnp.concatenate(faded, axis=0), vl, ((0,), (0,)))
        decay = jnp.exp(before)
        columns = dot(decay, jnp.ones((1, cv), F32), ((0,), (0,)), precision=HIGH)
        begin = jnp.where(first, slot_state[h * ck : (h + 1) * ck, :], 0.0)
        state = state + columns * begin
        state_out[h * ck : (h + 1) * ck, :] = state
        send_out[h * ck : (h + 1) * ck, :] = state.astype(BF16)
        send_out[hd * ck + h : hd * ck + h + 1, :ck] = decay.astype(BF16)
        decay_out[h : h + 1, :] = decay


def rest_specs(dims, consts):
    return [whole(c.shape) for c in consts], [whole(s.shape) for s in rest_outputs(dims)]


def rest_first(dims, normed, weights, down, consts, meta):
    hd = dims.heads
    const_specs, out_specs = rest_specs(dims, consts)
    n_const = len(consts)
    widest = max(w.shape[0] for w in weights) // dims.steps

    def body(meta_ref, normed_ref, wq, wql, wkl, wvl, down_ref, *refs):
        consts_in, outs = refs[:n_const], refs[n_const : n_const + 6]
        w_out, acc, wide, up_wide = refs[n_const + 6 :]
        step = pl.program_id(0)

        @pl.when(step == 0)
        def _():
            acc[...] = jnp.zeros_like(acc)

        unpack_weight(wq, wide, hd, dims.ca // 128, w_out, 0)
        unpack_weight(wql, wide, hd, dims.ck // 128, w_out, hd * dims.ca)
        unpack_weight(wkl, wide, hd, dims.ck // 128, w_out, hd * (dims.ca + dims.ck))
        unpack_weight(wvl, wide, hd, dims.cv // 128, w_out, hd * (dims.ca + 2 * dims.ck))
        at = pl.multiple_of(step * dims.chunk, dims.chunk)
        acc[...] += dot(normed_ref[:, pl.ds(at, dims.chunk)], w_out[...])

        @pl.when(step == dims.steps - 1)
        def _():
            low = dot(normed_ref[...], down_ref[...], ((1,), (1,))).astype(BF16)
            slot_state, up, bias, retain, query_gain = consts_in
            local_part(dims, acc, low, meta_ref, slot_state, up, up_wide, bias, retain, query_gain, outs)

    return pl.pallas_call(
        body,
        grid=(dims.steps,),
        in_specs=[SMEM, whole(normed.shape)]
        + [pl.BlockSpec((w.shape[0] // dims.steps, 128), lambda i: (i, 0)) for w in weights]
        + [whole(down.shape)]
        + const_specs,
        out_specs=out_specs + [pl.BlockSpec((dims.chunk, dims.rest), lambda i: (i, 0))],
        out_shape=rest_outputs(dims) + [jax.ShapeDtypeStruct((dims.model, dims.rest), BF16)],
        scratch_shapes=[
            pltpu.VMEM((dims.rows, dims.rest), F32),
            pltpu.VMEM((widest, 128), F32),
            pltpu.VMEM(consts[1].shape, F32),
        ],
        name="rest_first",
    )(meta, normed, *weights, down, *consts)


def rest_other(dims, normed, weights, down, consts, meta):
    const_specs, out_specs = rest_specs(dims, consts)
    n_const = len(consts)

    def body(meta_ref, normed_ref, w_ref, down_ref, *refs):
        consts_in, outs = refs[:n_const], refs[n_const : n_const + 6]
        acc, up_wide = refs[n_const + 6 :]
        acc[...] = dot(normed_ref[...], w_ref[...])
        low = dot(normed_ref[...], down_ref[...], ((1,), (1,))).astype(BF16)
        slot_state, up, bias, retain, query_gain = consts_in
        local_part(dims, acc, low, meta_ref, slot_state, up, up_wide, bias, retain, query_gain, outs)

    return pl.pallas_call(
        body,
        in_specs=[SMEM, whole(normed.shape), whole(weights.shape), whole(down.shape)] + const_specs,
        out_specs=out_specs,
        out_shape=rest_outputs(dims),
        scratch_shapes=[pltpu.VMEM((dims.rows, dims.rest), F32), pltpu.VMEM(consts[1].shape, F32)],
        name="rest_other",
    )(meta, normed, weights, down, *consts)


def columns_of(row, width):
    return dot(row, jnp.ones((1, width), row.dtype), ((0,), (0,)), precision=HIGH if row.dtype == F32 else None)


def combine(dims, bit, state, decay, prefix, prefix_decay, received, meta):
    hd, ck, cv = dims.heads, dims.ck, dims.cv

    def body(meta_ref, st, dec, pre, pre_dec, rec, send_out, st_out, dec_out, pre_out, pre_dec_out):
        upper = (meta_ref[0] // bit) % 2 == 1
        send_out[hd * ck :, :] = jnp.zeros((16, cv), BF16)
        dec_out[...] = jnp.ones_like(dec_out)
        pre_dec_out[...] = jnp.ones_like(pre_dec_out)
        for h in range(hd):
            at = slice(h * ck, (h + 1) * ck)
            other = rec[at, :].astype(F32)
            other_dec = rec[hd * ck + h : hd * ck + h + 1, :ck].astype(F32)
            mine, mine_dec = st[at, :], dec[h : h + 1, :]
            earlier = jnp.where(upper, other, mine)
            late = jnp.where(upper, mine, other)
            total = earlier * columns_of(jnp.where(upper, mine_dec, other_dec), cv) + late
            st_out[at, :] = total
            send_out[at, :] = total.astype(BF16)
            both = mine_dec * other_dec
            dec_out[h : h + 1, :] = both
            send_out[hd * ck + h : hd * ck + h + 1, :ck] = both.astype(BF16)
            pre_row = pre_dec[h : h + 1, :]
            pre_out[at, :] = pre[at, :] + jnp.where(upper, columns_of(pre_row, cv) * other, 0.0)
            pre_dec_out[h : h + 1, :] = jnp.where(upper, pre_row * other_dec, pre_row)

    shapes = [
        jax.ShapeDtypeStruct((hd * ck + 16, cv), BF16),
        jax.ShapeDtypeStruct((hd * ck, cv), F32),
        jax.ShapeDtypeStruct((16, ck), F32),
        jax.ShapeDtypeStruct((hd * ck, cv), F32),
        jax.ShapeDtypeStruct((16, ck), F32),
    ]
    args = (state, decay, prefix, prefix_decay, received)
    return pl.pallas_call(
        body,
        in_specs=[SMEM] + [whole(a.shape) for a in args],
        out_specs=[whole(s.shape) for s in shapes],
        out_shape=shapes,
        name="combine",
    )(meta, *args)


def finish(dims, bit, slot_index, kv_blocks, q_unit, reach, inside, prefix, prefix_decay, received, gains, lam, meta):
    hd, rows, ca, va, ck, cv = dims.heads, dims.rows, dims.ca, dims.va, dims.ck, dims.cv
    count = len(kv_blocks)
    mix_gain, state_gain = gains
    scale = (ca // 2) ** (-0.5)

    def body(meta_ref, lam_ref, *refs):
        kvs = refs[:count]
        q_ref, reach_ref, inside_ref, pre, pre_dec, rec, mix_ref, sg_ref, out = refs[count:]
        place = meta_ref[0]
        lane = lax.broadcasted_iota(jnp.int32, (rows, ca), 1)
        row_id = lax.broadcasted_iota(jnp.int32, (2 * rows, rows), 0) % rows
        col_id = lax.broadcasted_iota(jnp.int32, (2 * rows, rows), 1)
        allowed = row_id // BLK >= col_id // BLK
        upper = (place // bit) % 2 == 1
        for h in range(hd):
            q = q_ref[:, h * ca : (h + 1) * ca]
            zero = jnp.zeros_like(q)
            pair = jnp.concatenate([jnp.where(lane < ca // 2, q, zero), jnp.where(lane < ca // 2, zero, q)], axis=0)
            scores = []
            for m in range(count):
                s = dot(pair, kvs[m][:, h * ca : (h + 1) * ca], ((1,), (1,))) * scale
                if m == 0:
                    s = jnp.where(allowed, s, -jnp.inf)
                else:
                    s = jnp.where(jnp.bitwise_xor(place, m) < place, s, -jnp.inf)
                scores.append(s)
            top = functools.reduce(jnp.maximum, [jnp.max(s, axis=1, keepdims=True) for s in scores])
            total = jnp.zeros((2 * rows, 1), F32)
            sums = jnp.zeros((2 * rows, va), F32)
            for m in range(count):
                raised = jnp.exp(scores[m] - top)
                total = total + jnp.sum(raised, axis=1, keepdims=True)
                at = hd * ca + h * va
                sums = sums + dot(raised.astype(BF16), kvs[m][:, at : at + va])
            ratio = sums / total
            diff = ratio[:rows] - lam_ref[meta_ref[1] + h] * ratio[rows:]
            out[:, h * va : (h + 1) * va] = rms(diff, mix_ref[...]).astype(BF16)
            at = slice(h * ck, (h + 1) * ck)
            enter = pre[at, :]
            if rec is not None:
                more = columns_of(pre_dec[h : h + 1, :], cv) * rec[at, :].astype(F32)
                enter = enter + jnp.where(upper, more, 0.0)
            raw = inside_ref[:, h * cv : (h + 1) * cv] + dot(reach_ref[:, h * ck : (h + 1) * ck], enter.astype(BF16))
            at = hd * va + h * cv
            out[:, at : at + cv] = rms(raw, sg_ref[...]).astype(BF16)

    args = (*kv_blocks, q_unit, reach, inside, prefix, prefix_decay, received, mix_gain, state_gain)
    return pl.pallas_call(
        body,
        in_specs=[SMEM, SMEM] + [whole(a.shape) for a in args],
        out_specs=whole((rows, hd * (va + cv))),
        out_shape=jax.ShapeDtypeStruct((rows, hd * (va + cv)), BF16),
        name="finish",
    )(meta, lam, *args)


def project_out(dims, pieces, owners, weights, start):
    wa, wl = weights
    rows, cols = dims.rows, wa.shape[1]
    step_a, step_l = dims.heads * dims.va, dims.heads * dims.cv
    count = len(pieces)
    last = start is not None

    def body(own_ref, *refs):
        parts, (wa_ref, wl_ref) = refs[:count], refs[count : count + 2]
        out = refs[-1]
        total = refs[count + 2][...] if last else jnp.zeros((rows, cols), F32)
        for i in range(count):
            at = pl.multiple_of(own_ref[i] * step_a, step_a)
            total = total + dot(parts[i][:, :step_a], wa_ref[pl.ds(at, step_a), :])
            at = pl.multiple_of(own_ref[i] * step_l, step_l)
            total = total + dot(parts[i][:, step_a:], wl_ref[pl.ds(at, step_l), :])
        out[...] = total.astype(out.dtype)

    args = [*pieces, wa, wl] + ([start] if last else [])
    return pl.pallas_call(
        body,
        in_specs=[SMEM] + [whole(a.shape) for a in args],
        out_specs=whole((rows, cols)),
        out_shape=jax.ShapeDtypeStruct((rows, cols), BF16 if last else F32),
        name="project_last" if last else "project_own",
    )(owners, *args)


def swap(x, axis, bit, size):
    return lax.ppermute(x, axis, [(i, i ^ bit) for i in range(size)])


def shift(x, axis, by, size):
    return lax.ppermute(x, axis, [(i, (i + by) % size) for i in range(size)])


def low_bit(m):
    return m & -m


def body(
    tokens,
    norm_gain,
    query_attend,
    key_attend,
    value_attend,
    query_linear,
    key_linear,
    value_linear,
    decay_down,
    decay_up,
    decay_bias,
    log_retain,
    query_gain,
    key_gain,
    diff_lambda,
    mix_gain,
    state_gain,
    init_state,
    output_attend,
    output_linear,
):
    fs_size, tp_size, sp_size = (lax.axis_size(a) for a in ("fs", "tp", "sp"))
    fs, tp, sp = (lax.axis_index(a).astype(jnp.int32) for a in ("fs", "tp", "sp"))
    dims = Dims(tokens, query_attend, value_attend, key_linear, value_linear, decay_up)
    hd, rows, model = dims.heads, dims.rows, dims.model
    device = fs * tp_size + tp
    meta = jnp.stack([sp, device * hd, tp, fs])

    def flat(w):
        d, h, c = w.shape
        parts = c // 128
        return w.reshape(d, h, parts, 128).transpose(0, 2, 1, 3).reshape(d * parts * h, 128)

    own = tokens[0]
    retain_own = log_retain[0].T
    piece = rows // tp_size
    mine = lax.dynamic_slice_in_dim(own, tp * piece, piece, 0)
    token_parts, retains = [None], [retain_own]
    for j in range(1, fs_size):
        part = shift(mine, "fs", j, fs_size)
        retains.append(shift(retain_own, "fs", j, fs_size))
        token_parts.append([part] + [shift(part, "tp", -i, tp_size) for i in range(1, tp_size)])

    gain = norm_gain.reshape(1, -1)
    kg = key_gain.reshape(-1, key_gain.shape[-1])
    qg = query_gain.reshape(1, -1)
    up = decay_up.reshape(-1, decay_up.shape[-1])
    down = decay_down.T

    def consts(j):
        seq = (fs - j) % fs_size
        state = lax.dynamic_index_in_dim(init_state, seq, 0, False) if fs_size > 1 else init_state[0]
        return state.reshape(hd * dims.ck, dims.cv), up, decay_bias, retains[j], qg

    kv_blocks, results, states = [], [], []

    def spread(kv):
        blocks = [kv]
        for m in range(1, sp_size):
            blocks.append(swap(blocks[m - low_bit(m)] if m != low_bit(m) else kv, "sp", low_bit(m), sp_size))
        return blocks

    def prefix_of(j, outs, begin):
        _, _, _, send, state, decay = outs
        prefix = jnp.where(sp == 0, begin, 0.0)
        prefix_decay = jnp.ones((16, dims.ck), F32)
        bit = 1
        while True:
            received = swap(send, "sp", bit, sp_size)
            if bit * 2 >= sp_size:
                return bit, prefix, prefix_decay, received
            send, state, decay, prefix, prefix_decay = combine(
                dims, bit, state, decay, prefix, prefix_decay, received, meta
            )
            bit *= 2

    kv_w = rest_w = None
    for j in range(fs_size):
        if j == 0:
            kv, normed, kv_w = kv_first(dims, own, gain, flat(key_attend), flat(value_attend), kg, meta)
        else:
            kv, normed = kv_other(dims, token_parts[j], gain, kv_w, kg, meta)
        kv_blocks.append(spread(kv))
        c = consts(j)
        if j == 0:
            *outs, rest_w = rest_first(
                dims, normed, [flat(w) for w in (query_attend, query_linear, key_linear, value_linear)], down, c, meta
            )
        else:
            outs = rest_other(dims, normed, rest_w, down, c, meta)
        results.append(outs)
        states.append(prefix_of(j, outs, c[0]))

    gains = (mix_gain.reshape(1, -1), state_gain.reshape(1, -1))
    weights = (output_attend, output_linear)
    total = None
    late_pieces, late_owners = [], []
    for j in range(fs_size):
        bit, prefix, prefix_decay, received = states[j]
        q_unit, reach, inside = results[j][:3]
        mixed = finish(
            dims, bit, j, kv_blocks[j], q_unit, reach, inside, prefix, prefix_decay, received, gains, diff_lambda, meta
        )
        if j:
            mixed = shift(mixed, "fs", -j, fs_size)
        source = (fs + j) % fs_size
        pieces = [mixed] + [shift(mixed, "tp", -i, tp_size) for i in range(1, tp_size)]
        owners = [source * tp_size + (tp + i) % tp_size for i in range(tp_size)]
        if j == 0 and fs_size > 1:
            total = project_out(dims, pieces, jnp.stack(owners), weights, None)
        else:
            late_pieces += pieces
            late_owners += owners
    result = project_out(dims, late_pieces, jnp.stack(late_owners), weights, total)
    return result.reshape(1, rows, -1)


def solution(mesh):
    heads = P(None, ("fs", "tp"), None)
    positions = P(("grp", "fs"), "sp", None)
    in_specs = (
        positions,
        P(),
        heads,
        heads,
        heads,
        heads,
        heads,
        heads,
        P(),
        P(),
        P(),
        positions,
        P(),
        P(),
        P(),
        P(),
        P(),
        P("grp", ("fs", "tp"), None, None),
        P(None, "tp"),
        P(None, "tp"),
    )
    out_specs = P(("grp", "fs"), "sp", "tp")
    return jax.shard_map(body, mesh=mesh, in_specs=in_specs, out_specs=out_specs, check_vma=False)
```

```python
import functools

import jax
import jax.numpy as jnp
from jax import lax
from jax.experimental import pallas as pl
from jax.experimental.pallas import tpu as pltpu
from jax.sharding import PartitionSpec as P

EPS = 1e-06
TAU = 16.0
BLK = 64
F32 = jnp.float32
BF16 = jnp.bfloat16
HIGH = lax.Precision.HIGHEST


def dot(a, b, dims=((1,), (0,)), precision=None):
    return lax.dot_general(a, b, (dims, ((), ())), precision=precision, preferred_element_type=F32)


def rms(x, gain):
    return x * lax.rsqrt(jnp.mean(x * x, axis=-1, keepdims=True) + EPS) * gain


def rms_halves(x, gain):
    _, width = x.shape
    half = width // 2
    first = lax.broadcasted_iota(jnp.int32, x.shape, 1) < half
    sq = x * x
    low = jnp.sum(jnp.where(first, sq, 0.0), axis=-1, keepdims=True) / half
    high = jnp.sum(jnp.where(first, 0.0, sq), axis=-1, keepdims=True) / half
    return x * jnp.where(first, lax.rsqrt(low + EPS), lax.rsqrt(high + EPS)) * gain


def whole(shape, memory_space=pltpu.VMEM):
    return pl.BlockSpec(shape, lambda *_: (0,) * len(shape), memory_space=memory_space)


def params(mib):
    return pltpu.CompilerParams(vmem_limit_bytes=int(mib * 2**20))


def cost(us):
    return pl.CostEstimate(flops=int(us * COST_SCALE), transcendentals=0, bytes_accessed=0)


COST_SCALE = 2e8
FIRST_US = 8
FIRST_MIB = 56


def unpack_weight(w_ref, wide_ref, heads, parts, out_ref, column):
    rows = w_ref.shape[0] // (heads * parts)
    if heads * parts == 1:
        out_ref[:, column : column + 128] = w_ref[...]
        return
    wide_ref[: w_ref.shape[0], :] = w_ref[...].astype(F32)
    for head in range(heads):
        for part in range(parts):
            piece = wide_ref[pl.ds(part * heads + head, rows, stride=heads * parts), :]
            at = column + (head * parts + part) * 128
            out_ref[:, at : at + 128] = piece.astype(BF16)


class Dims:
    def __init__(self, tokens, query_attend, value_attend, key_linear, value_linear, decay_up):
        self.rows = tokens.shape[1]
        self.model = tokens.shape[2]
        self.heads = query_attend.shape[1]
        self.ca = query_attend.shape[2]
        self.va = value_attend.shape[2]
        self.ck = key_linear.shape[2]
        self.cv = value_linear.shape[2]
        self.all_heads = decay_up.shape[1]
        self.rank = decay_up.shape[0]
        self.kv = self.heads * (self.ca + self.va)
        self.rest = self.heads * (self.ca + 2 * self.ck + self.cv)
        self.steps = 4
        self.chunk = self.model // self.steps
        self.fs_size = lax.axis_size("fs")
        self.tp_size = lax.axis_size("tp")
        self.sp_size = lax.axis_size("sp")
        self.joined = self.heads * self.ca == self.cv
        self.state_at = 2 * self.rows if self.joined else 0

    def first_head(self):
        return (lax.axis_index("fs") * self.tp_size + lax.axis_index("tp")) * self.heads


class Fetch:
    def __init__(self, pairs, sems):
        self.copies = [pltpu.make_async_copy(src, dst, sems.at[i]) for i, (src, dst) in enumerate(pairs)]
        for copy in self.copies:
            copy.start()

    def wait(self, *which):
        for i in which:
            self.copies[i].wait()


HBM = pl.BlockSpec(memory_space=pltpu.HBM)


def like(x):
    return pltpu.VMEM(x.shape, x.dtype)


def call(body, us, mib, args, in_specs, outs, scratch, last_in_hbm=False):
    many = isinstance(outs, list)
    specs = [whole(o.shape) for o in outs] if many else whole(outs.shape)
    if last_in_hbm:
        specs[-1] = HBM
    return pl.pallas_call(
        body,
        in_specs=in_specs,
        out_specs=specs,
        out_shape=outs,
        scratch_shapes=scratch,
        compiler_params=params(mib),
        cost_estimate=cost(us),
    )(*args)


def write_kv(acc, key_gain, dims, outs):
    first = dims.first_head()
    rows, width = dims.rows, dims.heads * dims.ca
    for h in range(dims.heads):
        k = acc[:, h * dims.ca : (h + 1) * dims.ca].astype(BF16).astype(F32)
        row = 2 * (first + h)
        gain = jnp.concatenate([key_gain[pl.ds(row, 1), :], key_gain[pl.ds(row + 1, 1), :]], axis=1)
        k = rms_halves(k, gain).astype(BF16)
        for out in outs:
            out[:rows, h * dims.ca : (h + 1) * dims.ca] = k
    v = acc[:, width : width + dims.heads * dims.va].astype(BF16)
    for out in outs:
        out[rows : 2 * rows, :] = v


def chunks_of(raw_refs, dst_refs, steps):
    pairs = []
    for c in range(steps):
        for src, dst in zip(raw_refs, dst_refs):
            n = src.shape[0] // steps
            pairs.append((src.at[pl.ds(c * n, n), :], dst.at[pl.ds(c * n, n), :]))
    return pairs


def projected(normed_ref, raws, layout, dims, w_out, wide, fetch, first_copy, keep=None):
    acc = None
    for c in range(dims.steps):
        here = slice(c * dims.chunk, (c + 1) * dims.chunk)
        column = 0
        for i, (raw, parts) in enumerate(zip(raws, layout)):
            fetch.wait(first_copy + c * len(raws) + i)
            n = raw.shape[0] // dims.steps
            unpack_weight(
                raw.at[c * n : (c + 1) * n, :], wide.at[i % 2], dims.heads, parts, w_out.at[here, :], column
            )
            column += dims.heads * parts * 128
        if keep is not None:
            keep(here)
        part = dot(normed_ref[:, here], w_out[here, :])
        acc = part if acc is None else acc + part
    return acc


def slot_outputs(dims):
    hd, rows = dims.heads, dims.rows
    return [
        jax.ShapeDtypeStruct((rows, hd * dims.ca), BF16),
        jax.ShapeDtypeStruct((rows, hd * dims.ck), BF16),
        jax.ShapeDtypeStruct((rows, hd * dims.cv), F32),
        jax.ShapeDtypeStruct((2 * rows, hd * dims.ca), BF16),
        jax.ShapeDtypeStruct((dims.state_at + hd * dims.ck + 16, dims.cv), BF16),
        jax.ShapeDtypeStruct((hd * dims.ck, dims.cv), F32),
        jax.ShapeDtypeStruct((hd * dims.ck, dims.cv), F32),
        jax.ShapeDtypeStruct((hd * dims.ck, dims.cv), F32),
    ]


def slot_sequence(dims, slot):
    return lax.rem(lax.axis_index("fs") + dims.fs_size - slot, dims.fs_size)


def columns_of(row, width):
    return dot(row, jnp.ones((1, width), row.dtype), ((0,), (0,)), precision=HIGH if row.dtype == F32 else None)


def local_part(dims, slot, acc, base, low_rank, init, up, up_wide, bias, retain, query_gain, outs):
    q_out, reach_out, inside_out, _, send_out, state_out, decay_out, begin_out = outs
    state_at = dims.state_at
    hd, rows, ck, cv = dims.heads, dims.rows, dims.ck, dims.cv
    gain = jnp.concatenate([query_gain[...], query_gain[...]], axis=1)
    up_wide[...] = up[...].astype(F32)
    retain_columns = jnp.transpose(retain[...])
    head_lane = lax.broadcasted_iota(jnp.int32, retain_columns.shape, 1)
    row_id = lax.broadcasted_iota(jnp.int32, (rows, rows), 0)
    col_id = lax.broadcasted_iota(jnp.int32, (rows, rows), 1)
    same_block = row_id // BLK == col_id // BLK
    lower = row_id >= col_id
    summing = jnp.where(same_block & lower, 1.0, 0.0).astype(BF16)
    blocks = rows // BLK
    first = lax.axis_index("sp") == 0
    head0 = dims.first_head()
    sequence = slot_sequence(dims, slot)
    send_out[state_at + hd * ck :, :] = jnp.zeros((16, cv), BF16)
    for h in range(hd):
        q = acc[:, base + h * dims.ca : base + (h + 1) * dims.ca].astype(BF16).astype(F32)
        q_out[:, h * dims.ca : (h + 1) * dims.ca] = rms_halves(q, gain).astype(BF16)
    logs = []
    for h in range(hd):
        head = head0 + h
        up_head = up_wide[pl.ds(head, dims.rank, stride=dims.all_heads), :].astype(BF16)
        pre = dot(low_rank, up_head) + bias[pl.ds(head, 1), :]
        gate = jnp.minimum(pre, 0.0) - jnp.log1p(jnp.exp(-jnp.abs(pre)))
        kept = jnp.sum(jnp.where(head_lane == head, retain_columns, 0.0), axis=1, keepdims=True)
        logs.append(gate / TAU + kept)
    log_decay = jnp.concatenate(logs, axis=1)
    running = jnp.zeros_like(log_decay)
    left = log_decay
    for _ in range(3):
        term = left.astype(BF16)
        running = running + dot(summing, term)
        left = left - term.astype(F32)
    finals = [running[(b + 1) * BLK - 1 : (b + 1) * BLK, :] for b in range(blocks)]
    pivots = [running[b * BLK + BLK // 2 : b * BLK + BLK // 2 + 1, :] for b in range(blocks)]
    at = base + hd * dims.ca
    queries = acc[:, at : at + hd * ck].astype(BF16).astype(F32) * ck ** (-0.5)
    keys = acc[:, at + hd * ck : at + 2 * hd * ck].astype(BF16).astype(F32)
    q_edge, q_piv, k_piv, k_end, reach, faded = [], [], [], [], [], [None] * blocks
    before = jnp.zeros_like(finals[0])
    for b in range(blocks):
        here = slice(b * BLK, (b + 1) * BLK)
        run, q, k = running[here], queries[here], keys[here]
        q_edge.append(q * jnp.exp(run))
        q_piv.append((q * jnp.exp(run - pivots[b])).astype(BF16))
        k_piv.append((k * jnp.exp(pivots[b] - run)).astype(BF16))
        k_end.append(k * jnp.exp(finals[b] - run))
        reach.append((q_edge[b] * jnp.exp(before)).astype(BF16))
        reach_out[here, :] = reach[b]
        before = before + finals[b]
    later = jnp.zeros_like(finals[0])
    for b in range(blocks - 1, -1, -1):
        faded[b] = (k_end[b] * jnp.exp(later)).astype(BF16)
        later = later + finals[b]
    faded_rows = jnp.concatenate(faded, axis=0)
    decay = jnp.exp(before)
    for h in range(hd):
        of = slice(h * ck, (h + 1) * ck)
        at = base + hd * (dims.ca + 2 * ck) + h * cv
        vl = acc[:, at : at + cv].astype(BF16)
        for b in range(blocks):
            here = slice(b * BLK, (b + 1) * BLK)
            own = dot(q_piv[b][:, of], k_piv[b][:, of], ((1,), (1,)))
            own = jnp.where(lower[:BLK, :BLK], own, 0.0).astype(BF16)
            result = dot(own, vl[here])
            gap = jnp.zeros_like(finals[0][:, of])
            for c in range(b - 1, -1, -1):
                edge = (k_end[c][:, of] * jnp.exp(gap)).astype(BF16)
                across = dot(q_edge[b][:, of].astype(BF16), edge, ((1,), (1,)))
                result = result + dot(across.astype(BF16), vl[c * BLK : (c + 1) * BLK])
                gap = gap + finals[c][:, of]
            inside_out[here, h * cv : (h + 1) * cv] = result
        state = dot(faded_rows[:, of], vl, ((0,), (0,)))
        columns = columns_of(decay[:, of], cv)
        begin = init[pl.ds((sequence * hd + h) * ck, ck), :]
        begin = jnp.where(first, begin, 0.0)
        begin_out[of, :] = begin
        state = state + columns * begin
        state_out[of, :] = state
        decay_out[of, :] = columns
        send_out[state_at + h * ck : state_at + (h + 1) * ck, :] = state.astype(BF16)
        at = state_at + hd * ck + h
        send_out[at : at + 1, :ck] = decay[:, of].astype(BF16)


def slot_first(dims, tokens, gain, key_gain, weights, consts):
    parts = [dims.ca, dims.va, dims.ca, dims.ck, dims.ck, dims.cv]
    layout = [p // 128 for p in parts]
    n_const, n_out, n_w = len(consts), len(slot_outputs(dims)), len(weights)
    widest = max(w.shape[0] for w in weights) // dims.steps
    base = dims.kv

    def body(*refs):
        inputs, refs = refs[: 3 + n_w + n_const], refs[3 + n_w + n_const :]
        outs, packed, refs = refs[:n_out], refs[n_out], refs[n_out + 1 :]
        local, (normed, acc, w_out, wide, up_wide, sems, out_sems) = refs[: len(inputs)], refs[len(inputs) :]
        tok, gain_v, kg = local[:3]
        raws_v, consts_v = local[3 : 3 + n_w], local[3 + n_w :]
        pairs = list(zip(inputs[:2], local[:2])) + chunks_of(inputs[3 : 3 + n_w], raws_v, dims.steps)
        small = list(zip(inputs[2:3], local[2:3])) + list(zip(inputs[3 + n_w :], consts_v))
        fetch = Fetch(pairs + small, sems)
        fetch.wait(0, 1)
        normed[...] = rms(tok[...].astype(F32), gain_v[...]).astype(BF16)
        kept = []

        def keep(here):
            kept.append(pltpu.make_async_copy(w_out.at[here, :], packed.at[here, :], out_sems.at[len(kept)]))
            kept[-1].start()

        acc[...] = projected(normed, raws_v, layout, dims, w_out, wide, fetch, 2, keep)
        fetch.wait(*range(len(pairs), len(pairs) + len(small)))
        write_kv(acc, kg, dims, (outs[3], outs[4]) if dims.joined else (outs[3],))
        down, init, up, bias, retain, query_gain = consts_v
        low = dot(normed[...], down[...], ((1,), (1,))).astype(BF16)
        local_part(dims, 0, acc, base, low, init, up, up_wide, bias, retain, query_gain, outs)
        for copy in kept:
            copy.wait()

    args = (tokens, gain, key_gain, *weights, *consts)
    return call(
        body,
        FIRST_US,
        FIRST_MIB,
        args,
        [HBM] * len(args),
        slot_outputs(dims) + [jax.ShapeDtypeStruct((dims.model, dims.kv + dims.rest), BF16)],
        [like(a) for a in args]
        + [
            pltpu.VMEM(tokens.shape, BF16),
            pltpu.VMEM((dims.rows, dims.kv + dims.rest), F32),
            pltpu.VMEM((dims.model, dims.kv + dims.rest), BF16),
            pltpu.VMEM((2, widest, 128), F32),
            pltpu.VMEM(consts[2].shape, F32),
            pltpu.SemaphoreType.DMA((3 + n_w * dims.steps + n_const,)),
            pltpu.SemaphoreType.DMA((dims.steps,)),
        ],
        last_in_hbm=True,
    )


def slot_other(dims, slot, tokens, gain, key_gain, weights, consts):
    n_const, n_out = len(consts), len(slot_outputs(dims))
    base = dims.kv

    def body(tok, w_ref, *refs):
        small, refs = refs[: 2 + n_const], refs[2 + n_const :]
        outs, refs = refs[:n_out], refs[n_out:]
        local, (normed, acc, up_wide, sems) = refs[: 2 + n_const], refs[2 + n_const :]
        fetch = Fetch(list(zip(small, local)), sems)
        gain_v, kg = local[:2]
        fetch.wait(0)
        normed[...] = rms(tok[...].astype(F32), gain_v[...]).astype(BF16)
        acc[...] = dot(normed[...], w_ref[...])
        fetch.wait(*range(1, 2 + n_const))
        write_kv(acc, kg, dims, (outs[3], outs[4]) if dims.joined else (outs[3],))
        down, init, up, bias, retain, query_gain = local[2:]
        low = dot(normed[...], down[...], ((1,), (1,))).astype(BF16)
        local_part(dims, slot, acc, base, low, init, up, up_wide, bias, retain, query_gain, outs)

    args = (tokens, weights, gain, key_gain, *consts)
    return call(
        body,
        4,
        16,
        args,
        [whole(tokens.shape), whole(weights.shape)] + [HBM] * (2 + n_const),
        slot_outputs(dims),
        [like(a) for a in args[2:]]
        + [
            pltpu.VMEM(tokens.shape, BF16),
            pltpu.VMEM((dims.rows, dims.kv + dims.rest), F32),
            pltpu.VMEM(consts[2].shape, F32),
            pltpu.SemaphoreType.DMA((2 + n_const,)),
        ],
    )


def combine(dims, bit, state, decay, prefix, prefix_decay, received, base):
    hd, ck, cv = dims.heads, dims.ck, dims.cv
    begun = prefix_decay is not None

    def body(*refs):
        if begun:
            st, dec, pre, pre_dec, rec, send_out, st_out, dec_out, pre_out, pre_dec_out = refs
        else:
            st, dec, pre, rec, send_out, st_out, dec_out, pre_out, pre_dec_out = refs
        upper = lax.rem(lax.axis_index("sp") // bit, 2) == 1
        send_out[hd * ck :, :] = jnp.zeros((16, cv), BF16)
        for h in range(hd):
            at = slice(h * ck, (h + 1) * ck)
            other = rec[base + h * ck : base + (h + 1) * ck, :].astype(F32)
            other_row = rec[base + hd * ck + h : base + hd * ck + h + 1, :ck]
            other_dec = columns_of(other_row, cv)
            mine, mine_dec = st[at, :], dec[at, :]
            earlier = jnp.where(upper, other, mine)
            late = jnp.where(upper, mine, other)
            total = earlier * jnp.where(upper, mine_dec, other_dec) + late
            st_out[at, :] = total
            send_out[at, :] = total.astype(BF16)
            both = mine_dec * other_dec
            dec_out[at, :] = both
            if bit * 4 < dims.sp_size:
                send_out[hd * ck + h : hd * ck + h + 1, :ck] = jnp.transpose(both[:, :128])[:1, :].astype(BF16)
            if begun:
                pre_out[at, :] = pre[at, :] + jnp.where(upper, pre_dec[at, :] * other, 0.0)
                pre_dec_out[at, :] = jnp.where(upper, pre_dec[at, :] * other_dec, pre_dec[at, :])
            else:
                pre_out[at, :] = jnp.where(upper, other, pre[at, :])
                pre_dec_out[at, :] = jnp.where(upper, other_dec, 1.0)

    full = jax.ShapeDtypeStruct((hd * ck, cv), F32)
    args = (state, decay, prefix) + ((prefix_decay,) if begun else ()) + (received,)
    return call(
        body,
        2,
        6,
        args,
        [whole(a.shape) for a in args],
        [jax.ShapeDtypeStruct((hd * ck + 16, cv), BF16), full, full, full, full],
        [],
    )


def finish(dims, bit, kv_blocks, q_unit, reach, inside, prefix, prefix_decay, received, gains):
    hd, rows, ca, va, ck, cv = dims.heads, dims.rows, dims.ca, dims.va, dims.ck, dims.cv
    count = len(kv_blocks)
    scale = (ca // 2) ** (-0.5)

    def body(*refs):
        kvs = refs[:count]
        q_ref, reach_ref, inside_ref, pre, pre_dec, rec = refs[count : count + 6]
        gains_h, out, gains_v, sems = refs[count + 6 : count + 9], refs[count + 9], refs[count + 10 : -1], refs[-1]
        fetch = Fetch(list(zip(gains_h, gains_v)), sems)
        mix_ref, sg_ref, lam_ref = gains_v
        place = lax.axis_index("sp")
        head0 = dims.first_head()
        lane = lax.broadcasted_iota(jnp.int32, (rows, ca), 1)
        row_id = lax.rem(lax.broadcasted_iota(jnp.int32, (2 * rows, rows), 0), rows)
        col_id = lax.broadcasted_iota(jnp.int32, (2 * rows, rows), 1)
        allowed = row_id // BLK >= col_id // BLK
        upper = lax.rem(place // bit, 2) == 1
        raws, ratios = [], []
        for h in range(hd):
            at = slice(h * ck, (h + 1) * ck)
            enter = pre[at, :] + jnp.where(upper, pre_dec[at, :] * rec[at, :].astype(F32), 0.0)
            raws.append(inside_ref[:, h * cv : (h + 1) * cv] + dot(reach_ref[:, at], enter.astype(BF16)))
        for h in range(hd):
            q = q_ref[:, h * ca : (h + 1) * ca]
            zero = jnp.zeros_like(q)
            pair = jnp.concatenate([jnp.where(lane < ca // 2, q, zero), jnp.where(lane < ca // 2, zero, q)], axis=0)
            scores = []
            for m in range(count):
                s = dot(pair, kvs[m][:rows, h * ca : (h + 1) * ca], ((1,), (1,))) * scale
                if m == 0:
                    s = jnp.where(allowed, s, -jnp.inf)
                else:
                    s = jnp.where(jnp.bitwise_xor(place, m) < place, s, -jnp.inf)
                scores.append(s)
            top = jnp.max(functools.reduce(jnp.maximum, scores), axis=1, keepdims=True)
            total = jnp.zeros((2 * rows, rows), F32)
            sums = jnp.zeros((2 * rows, va), F32)
            for m in range(count):
                raised = jnp.exp(scores[m] - top)
                total = total + raised
                sums = sums + dot(raised.astype(BF16), kvs[m][rows : 2 * rows, h * va : (h + 1) * va])
            ratios.append(sums / jnp.sum(total, axis=1, keepdims=True))
        fetch.wait(0, 1, 2)
        lam_lane = lax.broadcasted_iota(jnp.int32, lam_ref.shape, 1)
        for h in range(hd):
            lam = jnp.sum(jnp.where(lam_lane == head0 + h, lam_ref[...], 0.0), axis=1, keepdims=True)
            diff = ratios[h][:rows] - lam * ratios[h][rows:]
            out[:, h * va : (h + 1) * va] = rms(diff, mix_ref[...]).astype(BF16)
            at = hd * va + h * cv
            out[:, at : at + cv] = rms(raws[h], sg_ref[...]).astype(BF16)

    args = (*kv_blocks, q_unit, reach, inside, prefix, prefix_decay, received)
    return call(
        body,
        3,
        10,
        args + gains,
        [whole(a.shape) for a in args] + [HBM] * 3,
        jax.ShapeDtypeStruct((rows, hd * (va + cv)), BF16),
        [like(g) for g in gains] + [pltpu.SemaphoreType.DMA((3,))],
    )


def project_out(dims, pieces, places, weights, start):
    wa, wl = weights
    rows, cols = dims.rows, wa.shape[1]
    step_a, step_l = dims.heads * dims.va, dims.heads * dims.cv
    count = len(pieces)
    last = start is not None

    def body(*refs):
        parts, (wa_h, wl_h), refs = refs[:count], refs[count : count + 2], refs[count + 2 :]
        begin = refs[0] if last else None
        out, a_v, l_v, sems = refs[1:] if last else refs
        pairs, fs, tp = [], lax.axis_index("fs"), lax.axis_index("tp")
        for i, (j, step) in enumerate(places):
            owner = lax.rem(fs + j, dims.fs_size) * dims.tp_size + lax.rem(tp + step, dims.tp_size)
            pairs.append((wa_h.at[pl.ds(pl.multiple_of(owner * step_a, step_a), step_a), :], a_v.at[i]))
            pairs.append((wl_h.at[pl.ds(pl.multiple_of(owner * step_l, step_l), step_l), :], l_v.at[i]))
        fetch = Fetch(pairs, sems)
        total = begin[...] if last else jnp.zeros((rows, cols), F32)
        for i in range(count):
            fetch.wait(2 * i)
            total = total + dot(parts[i][:, :step_a], a_v[i])
            fetch.wait(2 * i + 1)
            total = total + dot(parts[i][:, step_a:], l_v[i])
        out[...] = total.astype(out.dtype)

    starts = [start] if last else []
    return call(
        body,
        3,
        20,
        (*pieces, wa, wl, *starts),
        [whole(p.shape) for p in pieces] + [HBM] * 2 + [whole(s.shape) for s in starts],
        jax.ShapeDtypeStruct((rows, cols), BF16 if last else F32),
        [
            pltpu.VMEM((count, step_a, cols), BF16),
            pltpu.VMEM((count, step_l, cols), BF16),
            pltpu.SemaphoreType.DMA((2 * count,)),
        ],
    )


def swap(x, axis, bit, size):
    return lax.ppermute(x, axis, [(i, i ^ bit) for i in range(size)])


def shift(x, axis, by, size):
    return lax.ppermute(x, axis, [(i, (i + by) % size) for i in range(size)])


def low_bit(m):
    return m & -m


def body(
    tokens,
    norm_gain,
    query_attend,
    key_attend,
    value_attend,
    query_linear,
    key_linear,
    value_linear,
    decay_down,
    decay_up,
    decay_bias,
    log_retain,
    query_gain,
    key_gain,
    diff_lambda,
    mix_gain,
    state_gain,
    init_state,
    output_attend,
    output_linear,
):
    fs_size, tp_size, sp_size = (lax.axis_size(a) for a in ("fs", "tp", "sp"))
    dims = Dims(tokens, query_attend, value_attend, key_linear, value_linear, decay_up)
    rows = dims.rows

    def flat(w):
        d, h, c = w.shape
        parts = c // 128
        return w.reshape(d, h, parts, 128).transpose(0, 2, 1, 3).reshape(d * parts * h, 128)

    own = tokens[0]
    retain_own = log_retain[0].T
    gain = norm_gain.reshape(1, -1)
    kg = key_gain.reshape(-1, key_gain.shape[-1])
    up = decay_up.reshape(-1, decay_up.shape[-1])
    init = init_state.reshape(-1, dims.cv)
    token_slots = [own] + [shift(own, "fs", j, fs_size) for j in range(1, fs_size)]
    retains = [retain_own] + [shift(retain_own, "fs", j, fs_size) for j in range(1, fs_size)]

    def exchange(kv, send, state, decay, prefix):
        near = swap(send, "sp", 1, sp_size)
        blocks = [kv, near if dims.joined else swap(kv, "sp", 1, sp_size)]
        for m in range(2, sp_size):
            source = blocks[m - low_bit(m)]
            blocks.append(swap(source, "sp", low_bit(m), sp_size))
        prefix_decay = None
        received, base, bit = near, dims.state_at, 1
        while bit * 2 < sp_size:
            send, state, decay, prefix, prefix_decay = combine(
                dims, bit, state, decay, prefix, prefix_decay, received, base
            )
            bit, base = bit * 2, 0
            received = swap(send, "sp", bit, sp_size)
        return blocks, (bit, prefix, prefix_decay, received)

    all_weights = (key_attend, value_attend, query_attend, query_linear, key_linear, value_linear)
    results = []
    packed = None
    for j in range(fs_size):
        consts = (decay_down.T, init, up, decay_bias, retains[j], query_gain.reshape(1, -1))
        if j == 0:
            *outs, packed = slot_first(dims, own, gain, kg, [flat(w) for w in all_weights], consts)
        else:
            outs = slot_other(dims, j, token_slots[j], gain, kg, packed, consts)
        results.append((outs, exchange(*outs[3:])))

    gains = (mix_gain.reshape(1, -1), state_gain.reshape(1, -1), diff_lambda.reshape(1, -1))
    weights = (output_attend, output_linear)
    total = None
    pieces, places = [], []
    for j in range(fs_size):
        outs, (blocks, (bit, prefix, prefix_decay, received)) = results[j]
        mixed = finish(dims, bit, blocks, *outs[:3], prefix, prefix_decay, received, gains)
        if j:
            mixed = shift(mixed, "fs", -j, fs_size)
        arrived = [mixed] + [shift(mixed, "tp", -i, tp_size) for i in range(1, tp_size)]
        if j == 0 and fs_size > 1:
            total = project_out(dims, arrived, [(0, i) for i in range(tp_size)], weights, None)
        else:
            pieces += arrived
            places += [(j, i) for i in range(tp_size)]
    result = project_out(dims, pieces, places, weights, total)
    return result.reshape(1, rows, -1)


def solution(mesh):
    heads = P(None, ("fs", "tp"), None)
    positions = P(("grp", "fs"), "sp", None)
    in_specs = (
        positions,
        P(),
        heads,
        heads,
        heads,
        heads,
        heads,
        heads,
        P(),
        P(),
        P(),
        positions,
        P(),
        P(),
        P(),
        P(),
        P(),
        P("grp", ("fs", "tp"), None, None),
        P(None, "tp"),
        P(None, "tp"),
    )
    out_specs = P(("grp", "fs"), "sp", "tp")

    return jax.shard_map(body, mesh=mesh, in_specs=in_specs, out_specs=out_specs, check_vma=False)
```

```python
import functools

import jax
import jax.numpy as jnp
from jax import lax
from jax.experimental import pallas as pl
from jax.experimental.pallas import tpu as pltpu
from jax.sharding import PartitionSpec as P

EPS = 1e-06
TAU = 16.0
BLK = 64
F32 = jnp.float32
BF16 = jnp.bfloat16
HIGH = lax.Precision.HIGHEST


def dot(a, b, dims=((1,), (0,)), precision=None):
    return lax.dot_general(a, b, (dims, ((), ())), precision=precision, preferred_element_type=F32)


def rms(x, gain):
    return x * lax.rsqrt(jnp.mean(x * x, axis=-1, keepdims=True) + EPS) * gain


def rms_halves(x, gain):
    _, width = x.shape
    half = width // 2
    first = lax.broadcasted_iota(jnp.int32, x.shape, 1) < half
    sq = x * x
    low = jnp.sum(jnp.where(first, sq, 0.0), axis=-1, keepdims=True) / half
    high = jnp.sum(jnp.where(first, 0.0, sq), axis=-1, keepdims=True) / half
    return x * jnp.where(first, lax.rsqrt(low + EPS), lax.rsqrt(high + EPS)) * gain


def whole(shape, memory_space=pltpu.VMEM):
    return pl.BlockSpec(shape, lambda *_: (0,) * len(shape), memory_space=memory_space)


def params(mib):
    return pltpu.CompilerParams(vmem_limit_bytes=int(mib * 2**20))


def cost(us):
    return pl.CostEstimate(flops=int(us * COST_SCALE), transcendentals=0, bytes_accessed=0)


COST_SCALE = 2e8
LINGER_US = 40


def unpack_weight(w_ref, wide_ref, heads, parts, out_ref, column):
    rows = w_ref.shape[0] // (heads * parts)
    if heads * parts == 1:
        out_ref[:, column : column + 128] = w_ref[...]
        return
    wide_ref[: w_ref.shape[0], :] = w_ref[...].astype(F32)
    for head in range(heads):
        for part in range(parts):
            piece = wide_ref[pl.ds(part * heads + head, rows, stride=heads * parts), :]
            at = column + (head * parts + part) * 128
            out_ref[:, at : at + 128] = piece.astype(BF16)


class Dims:
    def __init__(self, tokens, query_attend, value_attend, key_linear, value_linear, decay_up):
        self.rows = tokens.shape[1]
        self.model = tokens.shape[2]
        self.heads = query_attend.shape[1]
        self.ca = query_attend.shape[2]
        self.va = value_attend.shape[2]
        self.ck = key_linear.shape[2]
        self.cv = value_linear.shape[2]
        self.all_heads = decay_up.shape[1]
        self.rank = decay_up.shape[0]
        self.steps = 4
        self.chunk = self.model // self.steps
        self.fs_size = lax.axis_size("fs")
        self.tp_size = lax.axis_size("tp")
        self.sp_size = lax.axis_size("sp")

    def first_head(self):
        return (lax.axis_index("fs") * self.tp_size + lax.axis_index("tp")) * self.heads


class Fetch:
    def __init__(self, pairs, sems, window=None):
        self.copies = [pltpu.make_async_copy(src, dst, sems.at[i]) for i, (src, dst) in enumerate(pairs)]
        self.started = 0
        self.window = len(pairs) if window is None else window
        self.start_to(self.window)

    def start_to(self, end):
        while self.started < min(end, len(self.copies)):
            self.copies[self.started].start()
            self.started += 1

    def wait(self, *which):
        for i in which:
            self.start_to(i + 1)
            self.copies[i].wait()
            self.start_to(i + 1 + self.window)


HBM = pl.BlockSpec(memory_space=pltpu.HBM)


def call(body, us, mib, args, in_specs, outs, scratch):
    many = isinstance(outs, list)
    specs = [whole(o.shape) for o in outs] if many else whole(outs.shape)
    return pl.pallas_call(
        body,
        in_specs=in_specs,
        out_specs=specs,
        out_shape=outs,
        scratch_shapes=scratch,
        compiler_params=params(mib),
        cost_estimate=cost(us),
    )(*args)


def write_kv(acc, key_gain, dims, out):
    first = dims.first_head()
    rows, width = dims.rows, dims.heads * dims.ca
    for h in range(dims.heads):
        k = acc[:, h * dims.ca : (h + 1) * dims.ca].astype(BF16).astype(F32)
        row = 2 * (first + h)
        gain = jnp.concatenate([key_gain[pl.ds(row, 1), :], key_gain[pl.ds(row + 1, 1), :]], axis=1)
        out[:rows, h * dims.ca : (h + 1) * dims.ca] = rms_halves(k, gain).astype(BF16)
    out[rows : 2 * rows, :] = acc[:, width : width + dims.heads * dims.va].astype(BF16)


def projected(normed_ref, raws, layout, dims, w_out, wide):
    acc = None
    for c in range(dims.steps):
        here = slice(c * dims.chunk, (c + 1) * dims.chunk)
        column = 0
        for i, (raw, parts) in enumerate(zip(raws, layout)):
            n = raw.shape[0] // dims.steps
            unpack_weight(
                raw.at[c * n : (c + 1) * n, :], wide.at[i % 2], dims.heads, parts, w_out.at[here, :], column
            )
            column += dims.heads * parts * 128
        part = dot(normed_ref[:, here], w_out[here, :])
        acc = part if acc is None else acc + part
    return acc


def work_scratch(dims, weights):
    width = sum(w.shape[0] for w in weights) // dims.model * 128
    widest = max(w.shape[0] for w in weights) // dims.steps
    return [
        pltpu.VMEM((dims.rows, width), F32),
        pltpu.VMEM((dims.model, width), BF16),
        pltpu.VMEM((2, widest, 128), F32),
    ]


def keys_work(dims, values, gain, weights, key_gain):
    layout = (dims.ca // 128, dims.va // 128)
    raw = gain is not None
    args = (values, *weights, key_gain) + ((gain,) if raw else ())

    def body(*refs):
        tok, weights_in, kg = refs[0], refs[1:3], refs[3]
        if raw:
            gain_ref, kv_out, normed, acc, w_out, wide = refs[4:]
            normed[...] = rms(tok[...].astype(F32), gain_ref[...]).astype(BF16)
        else:
            kv_out, acc, w_out, wide = refs[4:]
            normed = tok
        acc[...] = projected(normed, weights_in, layout, dims, w_out, wide)
        write_kv(acc, kg, dims, kv_out)

    kv = jax.ShapeDtypeStruct((2 * dims.rows, dims.heads * dims.ca), BF16)
    normed = jax.ShapeDtypeStruct(values.shape, BF16)
    outs = [kv] + ([normed] if raw else [])
    return call(
        body, 2, 12, args, [whole(a.shape) for a in args], outs, work_scratch(dims, weights)
    )


def slot_outputs(dims):
    hd, rows = dims.heads, dims.rows
    return [
        jax.ShapeDtypeStruct((rows, hd * dims.ca), BF16),
        jax.ShapeDtypeStruct((rows, hd * dims.ck), BF16),
        jax.ShapeDtypeStruct((rows, hd * dims.cv), F32),
        jax.ShapeDtypeStruct((hd * dims.ck + 16, dims.cv), BF16),
        jax.ShapeDtypeStruct((hd * dims.ck, dims.cv), F32),
        jax.ShapeDtypeStruct((hd * dims.ck, dims.cv), F32),
        jax.ShapeDtypeStruct((hd * dims.ck, dims.cv), F32),
    ]


def slot_sequence(dims, slot):
    return lax.rem(lax.axis_index("fs") + dims.fs_size - slot, dims.fs_size)


def columns_of(row, width):
    return dot(row, jnp.ones((1, width), row.dtype), ((0,), (0,)), precision=HIGH if row.dtype == F32 else None)


def local_part(dims, slot, acc, low_rank, init, up, up_wide, bias, retain, query_gain, outs):
    q_out, reach_out, inside_out, send_out, state_out, decay_out, begin_out = outs
    hd, rows, ck, cv = dims.heads, dims.rows, dims.ck, dims.cv
    gain = jnp.concatenate([query_gain[...], query_gain[...]], axis=1)
    up_wide[...] = up[...].astype(F32)
    retain_columns = jnp.transpose(retain[...])
    head_lane = lax.broadcasted_iota(jnp.int32, retain_columns.shape, 1)
    row_id = lax.broadcasted_iota(jnp.int32, (rows, rows), 0)
    col_id = lax.broadcasted_iota(jnp.int32, (rows, rows), 1)
    same_block = row_id // BLK == col_id // BLK
    lower = row_id >= col_id
    summing = jnp.where(same_block & lower, 1.0, 0.0).astype(BF16)
    blocks = rows // BLK
    first = lax.axis_index("sp") == 0
    head0 = dims.first_head()
    sequence = slot_sequence(dims, slot)
    send_out[hd * ck :, :] = jnp.zeros((16, cv), BF16)
    for h in range(hd):
        q = acc[:, h * dims.ca : (h + 1) * dims.ca].astype(BF16).astype(F32)
        q_out[:, h * dims.ca : (h + 1) * dims.ca] = rms_halves(q, gain).astype(BF16)
    logs = []
    for h in range(hd):
        head = head0 + h
        up_head = up_wide[pl.ds(head, dims.rank, stride=dims.all_heads), :].astype(BF16)
        pre = dot(low_rank, up_head) + bias[pl.ds(head, 1), :]
        gate = jnp.minimum(pre, 0.0) - jnp.log1p(jnp.exp(-jnp.abs(pre)))
        kept = jnp.sum(jnp.where(head_lane == head, retain_columns, 0.0), axis=1, keepdims=True)
        logs.append(gate / TAU + kept)
    log_decay = jnp.concatenate(logs, axis=1)
    running = jnp.zeros_like(log_decay)
    left = log_decay
    for _ in range(3):
        term = left.astype(BF16)
        running = running + dot(summing, term)
        left = left - term.astype(F32)
    finals = [running[(b + 1) * BLK - 1 : (b + 1) * BLK, :] for b in range(blocks)]
    pivots = [running[b * BLK + BLK // 2 : b * BLK + BLK // 2 + 1, :] for b in range(blocks)]
    at = hd * dims.ca
    queries = acc[:, at : at + hd * ck].astype(BF16).astype(F32) * ck ** (-0.5)
    keys = acc[:, at + hd * ck : at + 2 * hd * ck].astype(BF16).astype(F32)
    q_edge, q_piv, k_piv, k_end, reach, faded = [], [], [], [], [], [None] * blocks
    before = jnp.zeros_like(finals[0])
    for b in range(blocks):
        here = slice(b * BLK, (b + 1) * BLK)
        run, q, k = running[here], queries[here], keys[here]
        q_edge.append(q * jnp.exp(run))
        q_piv.append((q * jnp.exp(run - pivots[b])).astype(BF16))
        k_piv.append((k * jnp.exp(pivots[b] - run)).astype(BF16))
        k_end.append(k * jnp.exp(finals[b] - run))
        reach.append((q_edge[b] * jnp.exp(before)).astype(BF16))
        reach_out[here, :] = reach[b]
        before = before + finals[b]
    later = jnp.zeros_like(finals[0])
    for b in range(blocks - 1, -1, -1):
        faded[b] = (k_end[b] * jnp.exp(later)).astype(BF16)
        later = later + finals[b]
    faded_rows = jnp.concatenate(faded, axis=0)
    decay = jnp.exp(before)
    for h in range(hd):
        of = slice(h * ck, (h + 1) * ck)
        at = hd * (dims.ca + 2 * ck) + h * cv
        vl = acc[:, at : at + cv].astype(BF16)
        for b in range(blocks):
            here = slice(b * BLK, (b + 1) * BLK)
            own = dot(q_piv[b][:, of], k_piv[b][:, of], ((1,), (1,)))
            own = jnp.where(lower[:BLK, :BLK], own, 0.0).astype(BF16)
            result = dot(own, vl[here])
            gap = jnp.zeros_like(finals[0][:, of])
            for c in range(b - 1, -1, -1):
                edge = (k_end[c][:, of] * jnp.exp(gap)).astype(BF16)
                across = dot(q_edge[b][:, of].astype(BF16), edge, ((1,), (1,)))
                result = result + dot(across.astype(BF16), vl[c * BLK : (c + 1) * BLK])
                gap = gap + finals[c][:, of]
            inside_out[here, h * cv : (h + 1) * cv] = result
        state = dot(faded_rows[:, of], vl, ((0,), (0,)))
        columns = columns_of(decay[:, of], cv)
        begin = init[pl.ds((sequence * hd + h) * ck, ck), :]
        begin = jnp.where(first, begin, 0.0)
        begin_out[of, :] = begin
        state = state + columns * begin
        state_out[of, :] = state
        decay_out[of, :] = columns
        send_out[of, :] = state.astype(BF16)
        at = hd * ck + h
        send_out[at : at + 1, :ck] = decay[:, of].astype(BF16)


def rest_work(dims, slot, values, gain, weights, consts):
    layout = (dims.ca // 128, dims.ck // 128, dims.ck // 128, dims.cv // 128)
    raw = gain is not None
    n_out, n_in = len(slot_outputs(dims)), 1 + len(weights) + len(consts)
    args = (values, *weights, *consts) + ((gain,) if raw else ())

    def body(*refs):
        inputs, refs = refs[:n_in], refs[n_in:]
        tok, raws, consts_v = inputs[0], inputs[1 : 1 + len(weights)], inputs[1 + len(weights) :]
        if raw:
            gain_ref, refs = refs[0], refs[1:]
            outs, normed, (acc, w_out, wide, up_wide) = refs[:n_out], refs[n_out], refs[n_out + 1 :]
            normed[...] = rms(tok[...].astype(F32), gain_ref[...]).astype(BF16)
        else:
            outs, (acc, w_out, wide, up_wide) = refs[:n_out], refs[n_out:]
            normed = tok
        acc[...] = projected(normed, raws, layout, dims, w_out, wide)
        down, init, up, bias, retain, query_gain = consts_v
        low = dot(normed[...], down[...], ((1,), (1,))).astype(BF16)
        local_part(dims, slot, acc, low, init, up, up_wide, bias, retain, query_gain, outs)

    outs = slot_outputs(dims) + ([jax.ShapeDtypeStruct(values.shape, BF16)] if raw else [])
    scratch = work_scratch(dims, weights) + [pltpu.VMEM(consts[2].shape, F32)]
    return call(body, 4, 18, args, [whole(a.shape) for a in args], outs, scratch)


def linger(x):
    def body(x_ref, out):
        out[...] = x_ref[...]

    return call(body, LINGER_US, 1, (x,), [whole(x.shape)], jax.ShapeDtypeStruct(x.shape, x.dtype), [])


def combine(dims, bit, state, decay, prefix, prefix_decay, received):
    hd, ck, cv = dims.heads, dims.ck, dims.cv
    begun = prefix_decay is not None

    def body(*refs):
        if begun:
            st, dec, pre, pre_dec, rec, send_out, st_out, dec_out, pre_out, pre_dec_out = refs
        else:
            st, dec, pre, rec, send_out, st_out, dec_out, pre_out, pre_dec_out = refs
        upper = lax.rem(lax.axis_index("sp") // bit, 2) == 1
        send_out[hd * ck :, :] = jnp.zeros((16, cv), BF16)
        for h in range(hd):
            at = slice(h * ck, (h + 1) * ck)
            other = rec[at, :].astype(F32)
            other_row = rec[hd * ck + h : hd * ck + h + 1, :ck]
            other_dec = columns_of(other_row, cv)
            mine, mine_dec = st[at, :], dec[at, :]
            earlier = jnp.where(upper, other, mine)
            late = jnp.where(upper, mine, other)
            total = earlier * jnp.where(upper, mine_dec, other_dec) + late
            st_out[at, :] = total
            send_out[at, :] = total.astype(BF16)
            both = mine_dec * other_dec
            dec_out[at, :] = both
            if bit * 4 < dims.sp_size:
                send_out[hd * ck + h : hd * ck + h + 1, :ck] = jnp.transpose(both[:, :128])[:1, :].astype(BF16)
            if begun:
                pre_out[at, :] = pre[at, :] + jnp.where(upper, pre_dec[at, :] * other, 0.0)
                pre_dec_out[at, :] = jnp.where(upper, pre_dec[at, :] * other_dec, pre_dec[at, :])
            else:
                pre_out[at, :] = jnp.where(upper, other, pre[at, :])
                pre_dec_out[at, :] = jnp.where(upper, other_dec, 1.0)

    full = jax.ShapeDtypeStruct((hd * ck, cv), F32)
    args = (state, decay, prefix) + ((prefix_decay,) if begun else ()) + (received,)
    return call(
        body,
        2,
        6,
        args,
        [whole(a.shape) for a in args],
        [jax.ShapeDtypeStruct((hd * ck + 16, cv), BF16), full, full, full, full],
        [],
    )


def attend(dims, kv_blocks, q_unit, mix_gain, diff_lambda):
    hd, rows, ca, va = dims.heads, dims.rows, dims.ca, dims.va
    count = len(kv_blocks)
    scale = (ca // 2) ** (-0.5)

    def body(*refs):
        kvs = refs[:count]
        q_ref, mix_ref, lam_ref, out = refs[count:]
        place = lax.axis_index("sp")
        head0 = dims.first_head()
        lane = lax.broadcasted_iota(jnp.int32, (rows, ca), 1)
        row_id = lax.rem(lax.broadcasted_iota(jnp.int32, (2 * rows, rows), 0), rows)
        col_id = lax.broadcasted_iota(jnp.int32, (2 * rows, rows), 1)
        allowed = row_id // BLK >= col_id // BLK
        lam_lane = lax.broadcasted_iota(jnp.int32, lam_ref.shape, 1)
        for h in range(hd):
            q = q_ref[:, h * ca : (h + 1) * ca]
            zero = jnp.zeros_like(q)
            pair = jnp.concatenate([jnp.where(lane < ca // 2, q, zero), jnp.where(lane < ca // 2, zero, q)], axis=0)
            scores = []
            for m in range(count):
                s = dot(pair, kvs[m][:rows, h * ca : (h + 1) * ca], ((1,), (1,))) * scale
                if m == 0:
                    s = jnp.where(allowed, s, -jnp.inf)
                else:
                    s = jnp.where(jnp.bitwise_xor(place, m) < place, s, -jnp.inf)
                scores.append(s)
            top = jnp.max(functools.reduce(jnp.maximum, scores), axis=1, keepdims=True)
            total = jnp.zeros((2 * rows, rows), F32)
            sums = jnp.zeros((2 * rows, va), F32)
            for m in range(count):
                raised = jnp.exp(scores[m] - top)
                total = total + raised
                sums = sums + dot(raised.astype(BF16), kvs[m][rows : 2 * rows, h * va : (h + 1) * va])
            ratio = sums / jnp.sum(total, axis=1, keepdims=True)
            lam = jnp.sum(jnp.where(lam_lane == head0 + h, lam_ref[...], 0.0), axis=1, keepdims=True)
            diff = ratio[:rows] - lam * ratio[rows:]
            out[:, h * va : (h + 1) * va] = rms(diff, mix_ref[...]).astype(BF16)

    args = (*kv_blocks, q_unit, mix_gain, diff_lambda)
    out = jax.ShapeDtypeStruct((rows, hd * va), BF16)
    return call(body, 1.5, 8, args, [whole(a.shape) for a in args], out, [])


def recall(dims, bit, reach, inside, prefix, prefix_decay, received, state_gain):
    hd, rows, ck, cv = dims.heads, dims.rows, dims.ck, dims.cv

    def body(reach_ref, inside_ref, pre, pre_dec, rec, sg_ref, out):
        upper = lax.rem(lax.axis_index("sp") // bit, 2) == 1
        for h in range(hd):
            at, wide = slice(h * ck, (h + 1) * ck), slice(h * cv, (h + 1) * cv)
            enter = pre[at, :] + jnp.where(upper, pre_dec[at, :] * rec[at, :].astype(F32), 0.0)
            raw = inside_ref[:, wide] + dot(reach_ref[:, at], enter.astype(BF16))
            out[:, wide] = rms(raw, sg_ref[...]).astype(BF16)

    args = (reach, inside, prefix, prefix_decay, received, state_gain)
    out = jax.ShapeDtypeStruct((rows, hd * cv), BF16)
    return call(body, 1, 6, args, [whole(a.shape) for a in args], out, [])


def project_out(dims, pieces, weights, start, last):
    rows, cols = dims.rows, weights[0].shape[1]
    count = len(pieces)
    used = sorted({which for _, which, _, _ in pieces})

    def body(*refs):
        parts, mats, out = refs[:count], dict(zip(used, refs[count : count + len(used)])), refs[-1]
        fs, tp = lax.axis_index("fs"), lax.axis_index("tp")
        total = refs[count + len(used)][...] if start is not None else jnp.zeros((rows, cols), F32)
        for ref, (_, which, j, step) in zip(parts, pieces):
            owner = lax.rem(fs + j, dims.fs_size) * dims.tp_size + lax.rem(tp + step, dims.tp_size)
            size = ref.shape[1]
            at = pl.multiple_of(owner * size, size)
            total = total + dot(ref[...], mats[which][pl.ds(at, size), :])
        out[...] = total.astype(out.dtype)

    args = [p[0] for p in pieces] + [weights[w] for w in used] + ([] if start is None else [start])
    out = jax.ShapeDtypeStruct((rows, cols), BF16 if last else F32)
    return call(body, 1, 6, args, [whole(a.shape) for a in args], out, [])


def swap(x, axis, bit, size):
    return lax.ppermute(x, axis, [(i, i ^ bit) for i in range(size)])


def shift(x, axis, by, size):
    return lax.ppermute(x, axis, [(i, (i + by) % size) for i in range(size)])


def low_bit(m):
    return m & -m


def body(
    tokens,
    norm_gain,
    query_attend,
    key_attend,
    value_attend,
    query_linear,
    key_linear,
    value_linear,
    decay_down,
    decay_up,
    decay_bias,
    log_retain,
    query_gain,
    key_gain,
    diff_lambda,
    mix_gain,
    state_gain,
    init_state,
    output_attend,
    output_linear,
):
    fs_size, tp_size, sp_size = (lax.axis_size(a) for a in ("fs", "tp", "sp"))
    dims = Dims(tokens, query_attend, value_attend, key_linear, value_linear, decay_up)
    rows = dims.rows

    def flat(w):
        d, h, c = w.shape
        parts = c // 128
        return w.reshape(d, h, parts, 128).transpose(0, 2, 1, 3).reshape(d * parts * h, 128)

    own = tokens[0]
    retain_own = log_retain[0].T
    gain = norm_gain.reshape(1, -1)
    kg = key_gain.reshape(-1, key_gain.shape[-1])
    up = decay_up.reshape(-1, decay_up.shape[-1])
    init = init_state.reshape(-1, dims.cv)
    token_slots = [own] + [shift(own, "fs", j, fs_size) for j in range(1, fs_size)]
    retains = [retain_own] + [shift(retain_own, "fs", j, fs_size) for j in range(1, fs_size)]

    def keys_of_all(kv):
        blocks = [kv]
        for m in range(1, sp_size):
            blocks.append(swap(blocks[m - low_bit(m)], "sp", low_bit(m), sp_size))
        return blocks

    def entering(send, state, decay, prefix):
        prefix_decay, bit = None, 1
        while True:
            received = swap(send, "sp", bit, sp_size)
            if bit * 2 >= sp_size:
                return bit, prefix, prefix_decay, received
            send, state, decay, prefix, prefix_decay = combine(
                dims, bit, state, decay, prefix, prefix_decay, received
            )
            bit *= 2

    kv_weights = [flat(w) for w in (key_attend, value_attend)]
    rest_weights = [flat(w) for w in (query_attend, query_linear, key_linear, value_linear)]
    blocks, outs, states = [], [], []
    for j in range(fs_size):
        consts = (decay_down.T, init, up, decay_bias, retains[j], query_gain.reshape(1, -1))
        if j == 0:
            kv, normed = keys_work(dims, own, linger(gain), kv_weights, kg)
            out = rest_work(dims, j, normed, None, rest_weights, consts)
        else:
            *out, normed = rest_work(dims, j, token_slots[j], gain, rest_weights, consts)
            (kv,) = keys_work(dims, normed, None, kv_weights, kg)
        blocks.append(keys_of_all(kv))
        outs.append(out)
        states.append(entering(*out[3:]))

    mix, sg, lam = mix_gain.reshape(1, -1), state_gain.reshape(1, -1), diff_lambda.reshape(1, -1)
    weights = (output_attend, output_linear)
    early, late, last = [], [], []
    for j in range(fs_size):
        q_unit, reach, inside = outs[j][:3]
        bit, *entered = states[j]
        for which in range(2):
            if which == 0:
                value = attend(dims, blocks[j], q_unit, mix, lam)
            else:
                value = recall(dims, bit, reach, inside, *entered, sg)
            if j:
                value = shift(value, "fs", -j, fs_size)
            arrived = [value]
            arrived += [shift(value, "tp", -i, tp_size) for i in range(1, tp_size)]
            groups = [early] * tp_size if j else [late] + [last] * (tp_size - 1)
            for i, group in enumerate(groups):
                group.append((arrived[i], which, j, i))
    total = None
    groups = [(n, g) for n, g in (("early", early), ("late", late), ("last", last)) if g]
    for name, group in groups:
        total = project_out(dims, group, weights, total, name == groups[-1][0])
    return total.reshape(1, rows, -1)


def solution(mesh):
    heads = P(None, ("fs", "tp"), None)
    positions = P(("grp", "fs"), "sp", None)
    in_specs = (
        positions,
        P(),
        heads,
        heads,
        heads,
        heads,
        heads,
        heads,
        P(),
        P(),
        P(),
        positions,
        P(),
        P(),
        P(),
        P(),
        P(),
        P("grp", ("fs", "tp"), None, None),
        P(None, "tp"),
        P(None, "tp"),
    )
    out_specs = P(("grp", "fs"), "sp", "tp")

    return jax.shard_map(body, mesh=mesh, in_specs=in_specs, out_specs=out_specs, check_vma=False)
```

```python
import functools

import jax
import jax.numpy as jnp
from jax import lax
from jax.experimental import pallas as pl
from jax.experimental.pallas import tpu as pltpu
from jax.sharding import PartitionSpec as P

EPS = 1e-06
TAU = 16.0
BLK = 64
F32 = jnp.float32
BF16 = jnp.bfloat16
HIGH = lax.Precision.HIGHEST


def dot(a, b, dims=((1,), (0,)), precision=None):
    return lax.dot_general(a, b, (dims, ((), ())), precision=precision, preferred_element_type=F32)


def rms(x, gain):
    return x * lax.rsqrt(jnp.mean(x * x, axis=-1, keepdims=True) + EPS) * gain


def rms_halves(x, gain):
    _, width = x.shape
    half = width // 2
    first = lax.broadcasted_iota(jnp.int32, x.shape, 1) < half
    sq = x * x
    low = jnp.sum(jnp.where(first, sq, 0.0), axis=-1, keepdims=True) / half
    high = jnp.sum(jnp.where(first, 0.0, sq), axis=-1, keepdims=True) / half
    return x * jnp.where(first, lax.rsqrt(low + EPS), lax.rsqrt(high + EPS)) * gain


def whole(shape, memory_space=pltpu.VMEM):
    return pl.BlockSpec(shape, lambda *_: (0,) * len(shape), memory_space=memory_space)


def params(mib):
    return pltpu.CompilerParams(vmem_limit_bytes=int(mib * 2**20))


def cost(us):
    return pl.CostEstimate(flops=int(us * COST_SCALE), transcendentals=0, bytes_accessed=0)


COST_SCALE = 2e8
LINGER_US = 40


def unpack_weight(w_ref, wide_ref, heads, parts, out_ref, column):
    rows = w_ref.shape[0] // (heads * parts)
    if heads * parts == 1:
        out_ref[:, column : column + 128] = w_ref[...]
        return
    wide_ref[: w_ref.shape[0], :] = w_ref[...].astype(F32)
    for head in range(heads):
        for part in range(parts):
            piece = wide_ref[pl.ds(part * heads + head, rows, stride=heads * parts), :]
            at = column + (head * parts + part) * 128
            out_ref[:, at : at + 128] = piece.astype(BF16)


class Dims:
    def __init__(self, tokens, query_attend, value_attend, key_linear, value_linear, decay_up):
        self.rows = tokens.shape[1]
        self.model = tokens.shape[2]
        self.heads = query_attend.shape[1]
        self.ca = query_attend.shape[2]
        self.va = value_attend.shape[2]
        self.ck = key_linear.shape[2]
        self.cv = value_linear.shape[2]
        self.all_heads = decay_up.shape[1]
        self.rank = decay_up.shape[0]
        self.steps = 4
        self.chunk = self.model // self.steps
        self.fs_size = lax.axis_size("fs")
        self.tp_size = lax.axis_size("tp")
        self.sp_size = lax.axis_size("sp")

    def first_head(self):
        return (lax.axis_index("fs") * self.tp_size + lax.axis_index("tp")) * self.heads


class Fetch:
    def __init__(self, pairs, sems, window=None):
        self.copies = [pltpu.make_async_copy(src, dst, sems.at[i]) for i, (src, dst) in enumerate(pairs)]
        self.started = 0
        self.window = len(pairs) if window is None else window
        self.start_to(self.window)

    def start_to(self, end):
        while self.started < min(end, len(self.copies)):
            self.copies[self.started].start()
            self.started += 1

    def wait(self, *which):
        for i in which:
            self.start_to(i + 1)
            self.copies[i].wait()
            self.start_to(i + 1 + self.window)


HBM = pl.BlockSpec(memory_space=pltpu.HBM)


def call(body, us, mib, args, in_specs, outs, scratch):
    many = isinstance(outs, list)
    specs = [whole(o.shape) for o in outs] if many else whole(outs.shape)
    return pl.pallas_call(
        body,
        in_specs=in_specs,
        out_specs=specs,
        out_shape=outs,
        scratch_shapes=scratch,
        compiler_params=params(mib),
        cost_estimate=cost(us),
    )(*args)


def write_kv(acc, key_gain, dims, out):
    first = dims.first_head()
    rows, width = dims.rows, dims.heads * dims.ca
    for h in range(dims.heads):
        k = acc[:, h * dims.ca : (h + 1) * dims.ca].astype(BF16).astype(F32)
        row = 2 * (first + h)
        gain = jnp.concatenate([key_gain[pl.ds(row, 1), :], key_gain[pl.ds(row + 1, 1), :]], axis=1)
        out[:rows, h * dims.ca : (h + 1) * dims.ca] = rms_halves(k, gain).astype(BF16)
    out[rows : 2 * rows, :] = acc[:, width : width + dims.heads * dims.va].astype(BF16)


def projected(normed_ref, raws, layout, dims, w_out, wide):
    acc = None
    for c in range(dims.steps):
        here = slice(c * dims.chunk, (c + 1) * dims.chunk)
        column = 0
        for i, (raw, parts) in enumerate(zip(raws, layout)):
            n = raw.shape[0] // dims.steps
            unpack_weight(
                raw.at[c * n : (c + 1) * n, :], wide.at[i % 2], dims.heads, parts, w_out.at[here, :], column
            )
            column += dims.heads * parts * 128
        part = dot(normed_ref[:, here], w_out[here, :])
        acc = part if acc is None else acc + part
    return acc


def work_scratch(dims, weights):
    width = sum(w.shape[0] for w in weights) // dims.model * 128
    widest = max(w.shape[0] for w in weights) // dims.steps
    return [
        pltpu.VMEM((dims.rows, width), F32),
        pltpu.VMEM((dims.model, width), BF16),
        pltpu.VMEM((2, widest, 128), F32),
    ]


def keys_work(dims, values, gain, weights, key_gain):
    layout = (dims.ca // 128, dims.va // 128)
    raw = gain is not None
    args = (values, *weights, key_gain) + ((gain,) if raw else ())

    def body(*refs):
        tok, weights_in, kg = refs[0], refs[1:3], refs[3]
        if raw:
            gain_ref, kv_out, normed, acc, w_out, wide = refs[4:]
            normed[...] = rms(tok[...].astype(F32), gain_ref[...]).astype(BF16)
        else:
            kv_out, acc, w_out, wide = refs[4:]
            normed = tok
        acc[...] = projected(normed, weights_in, layout, dims, w_out, wide)
        write_kv(acc, kg, dims, kv_out)

    kv = jax.ShapeDtypeStruct((2 * dims.rows, dims.heads * dims.ca), BF16)
    normed = jax.ShapeDtypeStruct(values.shape, BF16)
    outs = [kv] + ([normed] if raw else [])
    return call(body, 2, 12, args, [whole(a.shape) for a in args], outs, work_scratch(dims, weights))


def slot_outputs(dims):
    hd, rows = dims.heads, dims.rows
    return [
        jax.ShapeDtypeStruct((rows, hd * dims.ca), BF16),
        jax.ShapeDtypeStruct((rows, hd * dims.ck), BF16),
        jax.ShapeDtypeStruct((rows, hd * dims.cv), F32),
        jax.ShapeDtypeStruct((hd * dims.ck + 16, dims.cv), BF16),
        jax.ShapeDtypeStruct((hd * dims.ck, dims.cv), F32),
        jax.ShapeDtypeStruct((hd * dims.ck, dims.cv), F32),
        jax.ShapeDtypeStruct((hd * dims.ck, dims.cv), F32),
    ]


def slot_sequence(dims, slot):
    return lax.rem(lax.axis_index("fs") + dims.fs_size - slot, dims.fs_size)


def columns_of(row, width):
    return dot(row, jnp.ones((1, width), row.dtype), ((0,), (0,)), precision=HIGH if row.dtype == F32 else None)


def local_part(dims, slot, acc, low_rank, init, up, up_wide, bias, retain, query_gain, outs):
    q_out, reach_out, inside_out, send_out, state_out, decay_out, begin_out = outs
    hd, rows, ck, cv = dims.heads, dims.rows, dims.ck, dims.cv
    gain = jnp.concatenate([query_gain[...], query_gain[...]], axis=1)
    up_wide[...] = up[...].astype(F32)
    retain_columns = jnp.transpose(retain[...])
    head_lane = lax.broadcasted_iota(jnp.int32, retain_columns.shape, 1)
    row_id = lax.broadcasted_iota(jnp.int32, (rows, rows), 0)
    col_id = lax.broadcasted_iota(jnp.int32, (rows, rows), 1)
    same_block = row_id // BLK == col_id // BLK
    lower = row_id >= col_id
    summing = jnp.where(same_block & lower, 1.0, 0.0).astype(BF16)
    blocks = rows // BLK
    first = lax.axis_index("sp") == 0
    head0 = dims.first_head()
    sequence = slot_sequence(dims, slot)
    send_out[hd * ck :, :] = jnp.zeros((16, cv), BF16)
    for h in range(hd):
        q = acc[:, h * dims.ca : (h + 1) * dims.ca].astype(BF16).astype(F32)
        q_out[:, h * dims.ca : (h + 1) * dims.ca] = rms_halves(q, gain).astype(BF16)
    logs = []
    for h in range(hd):
        head = head0 + h
        up_head = up_wide[pl.ds(head, dims.rank, stride=dims.all_heads), :].astype(BF16)
        pre = dot(low_rank, up_head) + bias[pl.ds(head, 1), :]
        gate = jnp.minimum(pre, 0.0) - jnp.log1p(jnp.exp(-jnp.abs(pre)))
        kept = jnp.sum(jnp.where(head_lane == head, retain_columns, 0.0), axis=1, keepdims=True)
        logs.append(gate / TAU + kept)
    log_decay = jnp.concatenate(logs, axis=1)
    running = jnp.zeros_like(log_decay)
    left = log_decay
    for _ in range(3):
        term = left.astype(BF16)
        running = running + dot(summing, term)
        left = left - term.astype(F32)
    finals = [running[(b + 1) * BLK - 1 : (b + 1) * BLK, :] for b in range(blocks)]
    pivots = [running[b * BLK + BLK // 2 : b * BLK + BLK // 2 + 1, :] for b in range(blocks)]
    at = hd * dims.ca
    queries = acc[:, at : at + hd * ck].astype(BF16).astype(F32) * ck ** (-0.5)
    keys = acc[:, at + hd * ck : at + 2 * hd * ck].astype(BF16).astype(F32)
    q_edge, q_piv, k_piv, k_end, reach, faded = [], [], [], [], [], [None] * blocks
    before = jnp.zeros_like(finals[0])
    for b in range(blocks):
        here = slice(b * BLK, (b + 1) * BLK)
        run, q, k = running[here], queries[here], keys[here]
        q_edge.append(q * jnp.exp(run))
        q_piv.append((q * jnp.exp(run - pivots[b])).astype(BF16))
        k_piv.append((k * jnp.exp(pivots[b] - run)).astype(BF16))
        k_end.append(k * jnp.exp(finals[b] - run))
        reach.append((q_edge[b] * jnp.exp(before)).astype(BF16))
        reach_out[here, :] = reach[b]
        before = before + finals[b]
    later = jnp.zeros_like(finals[0])
    for b in range(blocks - 1, -1, -1):
        faded[b] = (k_end[b] * jnp.exp(later)).astype(BF16)
        later = later + finals[b]
    faded_rows = jnp.concatenate(faded, axis=0)
    decay = jnp.exp(before)
    for h in range(hd):
        of = slice(h * ck, (h + 1) * ck)
        at = hd * (dims.ca + 2 * ck) + h * cv
        vl = acc[:, at : at + cv].astype(BF16)
        for b in range(blocks):
            here = slice(b * BLK, (b + 1) * BLK)
            own = dot(q_piv[b][:, of], k_piv[b][:, of], ((1,), (1,)))
            own = jnp.where(lower[:BLK, :BLK], own, 0.0).astype(BF16)
            result = dot(own, vl[here])
            gap = jnp.zeros_like(finals[0][:, of])
            for c in range(b - 1, -1, -1):
                edge = (k_end[c][:, of] * jnp.exp(gap)).astype(BF16)
                across = dot(q_edge[b][:, of].astype(BF16), edge, ((1,), (1,)))
                result = result + dot(across.astype(BF16), vl[c * BLK : (c + 1) * BLK])
                gap = gap + finals[c][:, of]
            inside_out[here, h * cv : (h + 1) * cv] = result
        state = dot(faded_rows[:, of], vl, ((0,), (0,)))
        columns = columns_of(decay[:, of], cv)
        begin = init[pl.ds((sequence * hd + h) * ck, ck), :]
        begin = jnp.where(first, begin, 0.0)
        begin_out[of, :] = begin
        state = state + columns * begin
        state_out[of, :] = state
        decay_out[of, :] = columns
        send_out[of, :] = state.astype(BF16)
        at = hd * ck + h
        send_out[at : at + 1, :ck] = decay[:, of].astype(BF16)


def rest_work(dims, slot, values, gain, weights, consts, after):
    layout = (dims.ca // 128, dims.ck // 128, dims.ck // 128, dims.cv // 128)
    raw = gain is not None
    n_out, n_in, n_v = len(slot_outputs(dims)), len(values) + len(weights) + len(consts), len(values)
    args = (*values, *weights, *consts, *after) + ((gain,) if raw else ())

    def body(*refs):
        inputs, refs = refs[:n_in], refs[n_in + len(after) :]
        toks, raws, consts_v = inputs[:n_v], inputs[n_v : n_v + len(weights)], inputs[n_v + len(weights) :]
        if raw:
            gain_ref, refs = refs[0], refs[1:]
            outs, normed, (acc, w_out, wide, up_wide) = refs[:n_out], refs[n_out], refs[n_out + 1 :]
            for i, tok in enumerate(toks):
                size = tok.shape[0]
                at = pl.multiple_of(lax.rem(lax.axis_index("tp") + i, n_v) * size, size) if n_v > 1 else 0
                normed[pl.ds(at, size), :] = rms(tok[...].astype(F32), gain_ref[...]).astype(BF16)
        else:
            outs, (acc, w_out, wide, up_wide) = refs[:n_out], refs[n_out:]
            normed = toks[0]
        acc[...] = projected(normed, raws, layout, dims, w_out, wide)
        down, init, up, bias, retain, query_gain = consts_v
        low = dot(normed[...], down[...], ((1,), (1,))).astype(BF16)
        local_part(dims, slot, acc, low, init, up, up_wide, bias, retain, query_gain, outs)

    outs = slot_outputs(dims) + ([jax.ShapeDtypeStruct((dims.rows, dims.model), BF16)] if raw else [])
    scratch = work_scratch(dims, weights) + [pltpu.VMEM(consts[2].shape, F32)]
    return call(body, 4, 18, args, [whole(a.shape) for a in args], outs, scratch)


def own_part(dims, tokens):
    size = dims.rows // dims.tp_size

    def body(tok, out):
        at = pl.multiple_of(lax.axis_index("tp") * size, size)
        out[...] = tok[pl.ds(at, size), :]

    out = jax.ShapeDtypeStruct((size, dims.model), BF16)
    return call(body, LINGER_US, 2, (tokens,), [whole(tokens.shape)], out, [])


def combine(dims, bit, state, decay, prefix, prefix_decay, received):
    hd, ck, cv = dims.heads, dims.ck, dims.cv
    begun, more = prefix_decay is not None, bit * 4 < dims.sp_size

    def body(*refs):
        if begun:
            st, dec, pre, pre_dec, rec, send_out, st_out, dec_out, pre_out, pre_dec_out = refs
        else:
            st, dec, pre, rec, send_out, st_out, dec_out, pre_out, pre_dec_out = refs
        upper = lax.rem(lax.axis_index("sp") // bit, 2) == 1
        if more:
            send_out[hd * ck :, :] = jnp.zeros((16, cv), BF16)
        for h in range(hd):
            at = slice(h * ck, (h + 1) * ck)
            other = rec[at, :].astype(F32)
            other_row = rec[hd * ck + h : hd * ck + h + 1, :ck]
            other_dec = columns_of(other_row, cv)
            mine, mine_dec = st[at, :], dec[at, :]
            earlier = jnp.where(upper, other, mine)
            late = jnp.where(upper, mine, other)
            total = earlier * jnp.where(upper, mine_dec, other_dec) + late
            st_out[at, :] = total
            send_out[at, :] = total.astype(BF16)
            both = mine_dec * other_dec
            dec_out[at, :] = both
            if more:
                send_out[hd * ck + h : hd * ck + h + 1, :ck] = jnp.transpose(both[:, :128])[:1, :].astype(BF16)
            if begun:
                pre_out[at, :] = pre[at, :] + jnp.where(upper, pre_dec[at, :] * other, 0.0)
                pre_dec_out[at, :] = jnp.where(upper, pre_dec[at, :] * other_dec, pre_dec[at, :])
            else:
                pre_out[at, :] = jnp.where(upper, other, pre[at, :])
                pre_dec_out[at, :] = jnp.where(upper, other_dec, 1.0)

    full = jax.ShapeDtypeStruct((hd * ck, cv), F32)
    args = (state, decay, prefix) + ((prefix_decay,) if begun else ()) + (received,)
    return call(
        body,
        2,
        6,
        args,
        [whole(a.shape) for a in args],
        [jax.ShapeDtypeStruct((hd * ck + (16 if more else 0), cv), BF16), full, full, full, full],
        [],
    )


def attend(dims, kv_blocks, q_unit, mix_gain, diff_lambda):
    hd, rows, ca, va = dims.heads, dims.rows, dims.ca, dims.va
    count = len(kv_blocks)
    scale = (ca // 2) ** (-0.5)

    def body(*refs):
        kvs = refs[:count]
        q_ref, mix_ref, lam_ref, out = refs[count:]
        place = lax.axis_index("sp")
        head0 = dims.first_head()
        lane = lax.broadcasted_iota(jnp.int32, (rows, ca), 1)
        row_id = lax.rem(lax.broadcasted_iota(jnp.int32, (2 * rows, rows), 0), rows)
        col_id = lax.broadcasted_iota(jnp.int32, (2 * rows, rows), 1)
        allowed = row_id // BLK >= col_id // BLK
        lam_lane = lax.broadcasted_iota(jnp.int32, lam_ref.shape, 1)
        for h in range(hd):
            q = q_ref[:, h * ca : (h + 1) * ca]
            zero = jnp.zeros_like(q)
            pair = jnp.concatenate([jnp.where(lane < ca // 2, q, zero), jnp.where(lane < ca // 2, zero, q)], axis=0)
            scores = []
            for m in range(count):
                s = dot(pair, kvs[m][:rows, h * ca : (h + 1) * ca], ((1,), (1,))) * scale
                if m == 0:
                    s = jnp.where(allowed, s, -jnp.inf)
                else:
                    s = jnp.where(jnp.bitwise_xor(place, m) < place, s, -jnp.inf)
                scores.append(s)
            top = jnp.max(functools.reduce(jnp.maximum, scores), axis=1, keepdims=True)
            total = jnp.zeros((2 * rows, rows), F32)
            sums = jnp.zeros((2 * rows, va), F32)
            for m in range(count):
                raised = jnp.exp(scores[m] - top)
                total = total + raised
                sums = sums + dot(raised.astype(BF16), kvs[m][rows : 2 * rows, h * va : (h + 1) * va])
            ratio = sums / jnp.sum(total, axis=1, keepdims=True)
            lam = jnp.sum(jnp.where(lam_lane == head0 + h, lam_ref[...], 0.0), axis=1, keepdims=True)
            diff = ratio[:rows] - lam * ratio[rows:]
            out[:, h * va : (h + 1) * va] = rms(diff, mix_ref[...]).astype(BF16)

    args = (*kv_blocks, q_unit, mix_gain, diff_lambda)
    out = jax.ShapeDtypeStruct((rows, hd * va), BF16)
    return call(body, 1.5, 8, args, [whole(a.shape) for a in args], out, [])


def recall(dims, bit, reach, inside, prefix, prefix_decay, received, state_gain):
    hd, rows, ck, cv = dims.heads, dims.rows, dims.ck, dims.cv

    def body(reach_ref, inside_ref, pre, pre_dec, rec, sg_ref, out):
        upper = lax.rem(lax.axis_index("sp") // bit, 2) == 1
        for h in range(hd):
            at, wide = slice(h * ck, (h + 1) * ck), slice(h * cv, (h + 1) * cv)
            enter = pre[at, :] + jnp.where(upper, pre_dec[at, :] * rec[at, :].astype(F32), 0.0)
            raw = inside_ref[:, wide] + dot(reach_ref[:, at], enter.astype(BF16))
            out[:, wide] = rms(raw, sg_ref[...]).astype(BF16)

    args = (reach, inside, prefix, prefix_decay, received, state_gain)
    out = jax.ShapeDtypeStruct((rows, hd * cv), BF16)
    return call(body, 1, 6, args, [whole(a.shape) for a in args], out, [])


def project_out(dims, pieces, weights, start, last):
    rows, cols = dims.rows, weights[0].shape[1]
    count = len(pieces)
    used = sorted({which for _, which, _, _ in pieces})

    def body(*refs):
        parts, mats, out = refs[:count], dict(zip(used, refs[count : count + len(used)])), refs[-1]
        fs, tp = lax.axis_index("fs"), lax.axis_index("tp")
        total = refs[count + len(used)][...] if start is not None else jnp.zeros((rows, cols), F32)
        for ref, (_, which, j, step) in zip(parts, pieces):
            owner = lax.rem(fs + j, dims.fs_size) * dims.tp_size + lax.rem(tp + step, dims.tp_size)
            size = ref.shape[1]
            at = pl.multiple_of(owner * size, size)
            total = total + dot(ref[...], mats[which][pl.ds(at, size), :])
        out[...] = total.astype(out.dtype)

    args = [p[0] for p in pieces] + [weights[w] for w in used] + ([] if start is None else [start])
    out = jax.ShapeDtypeStruct((rows, cols), BF16 if last else F32)
    return call(body, 1, 6, args, [whole(a.shape) for a in args], out, [])


def swap(x, axis, bit, size):
    return lax.ppermute(x, axis, [(i, i ^ bit) for i in range(size)])


def shift(x, axis, by, size):
    return lax.ppermute(x, axis, [(i, (i + by) % size) for i in range(size)])


def shift_both(x, j, i, fs_size, tp_size):
    places = [(f, t) for f in range(fs_size) for t in range(tp_size)]
    perm = [(f * tp_size + t, (f - j) % fs_size * tp_size + (t - i) % tp_size) for f, t in places]
    return lax.ppermute(x, ("fs", "tp"), perm)


def low_bit(m):
    return m & -m


def body(
    tokens,
    norm_gain,
    query_attend,
    key_attend,
    value_attend,
    query_linear,
    key_linear,
    value_linear,
    decay_down,
    decay_up,
    decay_bias,
    log_retain,
    query_gain,
    key_gain,
    diff_lambda,
    mix_gain,
    state_gain,
    init_state,
    output_attend,
    output_linear,
):
    fs_size, tp_size, sp_size = (lax.axis_size(a) for a in ("fs", "tp", "sp"))
    dims = Dims(tokens, query_attend, value_attend, key_linear, value_linear, decay_up)
    rows = dims.rows

    def flat(w):
        d, h, c = w.shape
        parts = c // 128
        return w.reshape(d, h, parts, 128).transpose(0, 2, 1, 3).reshape(d * parts * h, 128)

    own = tokens[0]
    retain_own = log_retain[0].T
    gain = norm_gain.reshape(1, -1)
    kg = key_gain.reshape(-1, key_gain.shape[-1])
    up = decay_up.reshape(-1, decay_up.shape[-1])
    init = init_state.reshape(-1, dims.cv)
    mine = own_part(dims, own)
    token_slots = [(own,)]
    for j in range(1, fs_size):
        part = shift(mine, "fs", j, fs_size)
        token_slots.append((part, *(shift(part, "tp", -i, tp_size) for i in range(1, tp_size))))
    retains = [retain_own] + [shift(retain_own, "fs", j, fs_size) for j in range(1, fs_size)]

    def keys_of_all(kv):
        blocks = [kv]
        for m in range(1, sp_size):
            blocks.append(swap(blocks[m - low_bit(m)], "sp", low_bit(m), sp_size))
        return blocks

    def entering(send, state, decay, prefix):
        prefix_decay, bit = None, 1
        while True:
            received = swap(send, "sp", bit, sp_size)
            if bit * 2 >= sp_size:
                return bit, prefix, prefix_decay, received
            send, state, decay, prefix, prefix_decay = combine(
                dims, bit, state, decay, prefix, prefix_decay, received
            )
            bit *= 2

    kv_weights = [flat(w) for w in (key_attend, value_attend)]
    rest_weights = [flat(w) for w in (query_attend, query_linear, key_linear, value_linear)]
    blocks, outs, states = [], [], []
    for j in range(fs_size):
        consts = (decay_down.T, init, up, decay_bias, retains[j], query_gain.reshape(1, -1))
        after = () if j else (mine,)
        *out, normed = rest_work(dims, j, token_slots[j], gain, rest_weights, consts, after)
        (kv,) = keys_work(dims, normed, None, kv_weights, kg)
        blocks.append(keys_of_all(kv))
        outs.append(out)
        states.append(entering(*out[3:]))

    mix, sg, lam = mix_gain.reshape(1, -1), state_gain.reshape(1, -1), diff_lambda.reshape(1, -1)
    weights = (output_attend, output_linear)
    early, late = [], []
    for j in range(fs_size):
        q_unit, reach, inside = outs[j][:3]
        bit, *entered = states[j]
        for which in range(2):
            if which == 0:
                value = attend(dims, blocks[j], q_unit, mix, lam)
            else:
                value = recall(dims, bit, reach, inside, *entered, sg)
            arrived = [value]
            if j:
                arrived = [shift(value, "fs", -j, fs_size)]
            for i in range(1, tp_size):
                if j and which == 0:
                    arrived.append(shift_both(value, j, i, fs_size, tp_size))
                else:
                    arrived.append(shift(arrived[0], "tp", -i, tp_size))
            for i in range(tp_size):
                soon = i == 0 and (j == 0 or which == 1)
                (early if soon else late).append((arrived[i], which, j, i))
    total = None
    groups = [("early", early), ("late", late)]
    for name, group in groups:
        total = project_out(dims, group, weights, total, name == groups[-1][0])
    return total.reshape(1, rows, -1)


def solution(mesh):
    heads = P(None, ("fs", "tp"), None)
    positions = P(("grp", "fs"), "sp", None)
    in_specs = (
        positions,
        P(),
        heads,
        heads,
        heads,
        heads,
        heads,
        heads,
        P(),
        P(),
        P(),
        positions,
        P(),
        P(),
        P(),
        P(),
        P(),
        P("grp", ("fs", "tp"), None, None),
        P(None, "tp"),
        P(None, "tp"),
    )
    out_specs = P(("grp", "fs"), "sp", "tp")

    return jax.shard_map(body, mesh=mesh, in_specs=in_specs, out_specs=out_specs, check_vma=False)
```
